512 devices in a mesh: kv: 64 (over z, y), tp: 8 (over x, core).
Axes of the slice: x: 4, y: 4, z: 16, core: 2. Of those that a mesh axis runs over, the one named last changes fastest.
Arguments:
- tokens: bfloat16 [16384, 2048], P('kv'), may hold values from -72 to 72
- w_query: bfloat16 [2048, 1024], P(None, 'tp'), may hold values from -0.125 to 0.125
- w_key: bfloat16 [2048, 1024], P(None, 'tp'), may hold values from -0.125 to 0.125
- w_value: bfloat16 [2048, 1024], P(None, 'tp'), may hold values from -0.125 to 0.125
- w_out: bfloat16 [1024, 2048], P('tp'), may hold values from -0.1875 to 0.1875
- chosen: int32 [256, 16], replicated, may hold values from -1 to 255, as said below
Outputs:
- mixed: bfloat16 [16384, 2048], P(('kv', 'tp'))
- log_sums: float32 [16, 16384], P('tp', 'kv')
The draws below stay inside these ranges and needn't reach their ends.
Inputs may be any that keep to these rules, and one draw needn't show every extreme that they name: `chosen`: row b begins with b itself, then lists distinct key blocks at most b, then holds -1 in its remaining entries. Taken together, the rows of the query blocks of one index of kv list at most 2 distinct blocks of the positions of any other index of kv, and exactly 2 for some pairs of indices in every draw.
All inputs are finite; a program needn't handle non-finite values.
Results may differ from the reference program's by a relative error of at most 0.03.
Values may be sent and summed in bfloat16 or wider, within the bound.
No kernel may reach another device: no remote copies, remote signals or barrier semaphores. Data moves between devices by JAX's collectives and lax.ppermute only.
A program may use at most 64 MiB of HBM per device.

```python
import jax
import jax.numpy as jnp
from jax import lax

D = 2048
HEADS = 16
HEAD_DIM = 64
BLK = 64
SEL = 16
CAP = 2
TOK_DEV = 256
ATT = 1024
TOKENS = 16384
NBLK = 256
N_TP = 8


def draw_tokens(key, part):
    values = jnp.clip(jax.random.normal(key, (TOKENS, D), jnp.float32), -6.0, 6.0)
    return values.astype(jnp.bfloat16)


def draw_chosen(key, part):
    per_dev = TOK_DEV // BLK
    devices = NBLK // per_dev
    pair_key = jax.random.fold_in(key, 11)
    hot_key = jax.random.fold_in(key, 12)
    rank_key = jax.random.fold_in(key, 13)
    order_bits = jax.random.randint(pair_key, (devices, devices, per_dev), 0, 1 << 20) * per_dev + jnp.arange(per_dev)
    ordering = jnp.argsort(order_bits, axis=-1)[..., :CAP]
    picked_blocks = jnp.arange(devices)[None, :, None] * per_dev + ordering
    hotness = jax.random.randint(hot_key, (devices,), 0, 4)
    blocks = jnp.arange(NBLK)
    query_block = blocks[:, None]
    target = blocks[None, :]
    query_dev = query_block // per_dev
    target_dev = target // per_dev
    pair_table = jnp.any(picked_blocks[:, blocks // per_dev, :] == blocks[None, :, None], axis=-1)
    in_pair = pair_table[blocks // per_dev] & (target_dev < query_dev)
    same_dev = (target_dev == query_dev) & (target <= query_block)
    near_dev = (target_dev == query_dev - 1) | (target_dev == query_dev - devices // 2)
    tier_level = jnp.where(target == query_block, 3, jnp.where(same_dev | in_pair & near_dev, 2, 1))
    jitter = jax.random.randint(rank_key, (NBLK, NBLK), 0, 1 << 12)
    rating = ((tier_level * 4 + hotness[target_dev]) * 4096 + jitter) * NBLK + target
    rating = jnp.where(same_dev | in_pair, rating, -1 - target)
    values, position = lax.top_k(rating, SEL)
    return jnp.where(values >= 0, position, -1).astype(jnp.int32)


def level_of(stream_key, extent, split, smallest, high):
    gain = 1.0
    for dim, blocks in split:
        steps = jax.random.uniform(jax.random.fold_in(jax.random.fold_in(stream_key, 6), dim), (blocks,), jnp.float32, smallest / len(split), high / len(split))
        gain = gain * jnp.repeat(jnp.exp(steps), extent[dim] // blocks).reshape((-1,) + (1,) * (len(extent) - 1 - dim))
    return gain


def normal_values(stream_key, shape, deviation, reach, cuts=(), held_as=jnp.bfloat16):
    result = deviation * jax.random.normal(stream_key, shape, jnp.float32)
    if cuts:
        result = result * level_of(stream_key, shape, cuts, -0.22, 0.18)
    return jnp.clip(result, -reach, reach).astype(held_as)


def setup_inputs(seed: int = 0) -> dict:
    keys = jax.random.split(jax.random.key(seed), 7)
    tokens = draw_tokens(jax.random.fold_in(keys[6], 71), 0)
    w_query = normal_values(keys[1], (D, ATT), D ** -0.5, 0.125, ((1, 8),))
    w_key = normal_values(keys[2], (D, ATT), D ** -0.5, 0.125, ((1, 8),))
    w_value = normal_values(keys[3], (D, ATT), D ** -0.5, 0.125, ((1, 8),))
    w_out = normal_values(keys[4], (ATT, D), ATT ** -0.5, 0.1875, ((0, 8),))
    chosen = draw_chosen(jax.random.fold_in(keys[6], 71), 0)
    return dict(tokens=tokens, w_query=w_query, w_key=w_key, w_value=w_value, w_out=w_out, chosen=chosen)


rotary_base = 500000.0
masked_score = -1e30


def rotate(values, positions, head_count, head_size):
    half_size = head_size // 2
    inverse = rotary_base ** (-jnp.arange(half_size, dtype=jnp.float32) / half_size)
    angles = positions.astype(jnp.float32)[:, None, None] * inverse[None, None, :]
    cos_part = jnp.cos(angles)
    sin_part = jnp.sin(angles)
    grouped = values.reshape(values.shape[0], head_count, head_size)
    first_half = grouped[..., :half_size]
    second_half = grouped[..., half_size:]
    turned = jnp.concatenate([first_half * cos_part - second_half * sin_part, second_half * cos_part + first_half * sin_part], axis=-1)
    return turned.reshape(values.shape)


def reference(tokens, w_query, w_key, w_value, w_out, chosen):
    positions = jnp.arange(TOKENS)
    query = rotate(jnp.dot(tokens, w_query, preferred_element_type=jnp.float32), positions, HEADS, HEAD_DIM).astype(jnp.bfloat16)
    keys_all = rotate(jnp.dot(tokens, w_key, preferred_element_type=jnp.float32), positions, HEADS, HEAD_DIM).astype(jnp.bfloat16)
    values_all = jnp.dot(tokens, w_value, preferred_element_type=jnp.float32).astype(jnp.bfloat16)
    key_blocks = keys_all.reshape(NBLK, BLK, HEADS, HEAD_DIM)
    value_blocks = values_all.reshape(NBLK, BLK, HEADS, HEAD_DIM)
    query_blocks = query.reshape(NBLK, BLK, HEADS, HEAD_DIM)
    scaling = HEAD_DIM ** -0.5

    def one_block(inputs):
        query_rows, listed = inputs
        usable = listed >= 0
        safe_rows = jnp.maximum(listed, 0)
        picked_keys = key_blocks[safe_rows].reshape(SEL * BLK, HEADS, HEAD_DIM)
        picked_values = value_blocks[safe_rows].reshape(SEL * BLK, HEADS, HEAD_DIM)
        scores = jnp.einsum('qhd,khd->hqk', query_rows.astype(jnp.float32), picked_keys.astype(jnp.float32)) * scaling
        key_mask = jnp.broadcast_to(usable[:, None], (SEL, BLK)).reshape(SEL * BLK)
        scores = jnp.where(key_mask[None, None, :], scores, masked_score)
        row_max = jnp.max(scores, axis=-1)
        weights = jnp.where(key_mask[None, None, :], jnp.exp(scores - row_max[..., None]), 0.0)
        totals = jnp.sum(weights, axis=-1)
        rounded = lax.optimization_barrier(weights.astype(jnp.bfloat16)).astype(jnp.float32)
        summed = jnp.einsum('hqk,khd->qhd', rounded, picked_values.astype(jnp.float32))
        mixed_rows = (summed / jnp.transpose(totals)[:, :, None]).reshape(BLK, HEADS * HEAD_DIM).astype(jnp.bfloat16)
        return mixed_rows, row_max + jnp.log(totals)

    mixed_all, log_blocks = lax.map(one_block, (query_blocks, chosen))
    attended = mixed_all.reshape(TOKENS, HEADS * HEAD_DIM)
    log_sums = jnp.transpose(log_blocks, (1, 0, 2)).reshape(HEADS, TOKENS)
    group_width = HEADS * HEAD_DIM // N_TP
    output = jnp.zeros((TOKENS, D), jnp.float32)
    for group_index in range(N_TP):
        lower = group_index * group_width
        partial_sum = jnp.dot(attended[:, lower:lower + group_width], w_out[lower:lower + group_width], preferred_element_type=jnp.float32)
        output = output + lax.optimization_barrier(partial_sum.astype(jnp.bfloat16)).astype(jnp.float32)
    return output.astype(jnp.bfloat16), log_sums
```

```python
import functools

import jax
import jax.numpy as jnp
from jax import lax
from jax.experimental import pallas as pl
from jax.experimental.pallas import tpu as pltpu
from jax.sharding import Mesh
from jax.sharding import PartitionSpec as P

HEAD_DIM = 64
BLK = 64
SEL = 16
ROWS = 256
PER = 4
WIDTH = 128
RING = 8
TEAM = 8
QB = TEAM * PER
MAXP = QB * SEL
UNROLL = 8
STATS = 16

rotary_base = 500000.0
masked_score = -1e30
f32 = jnp.float32
bf16 = jnp.bfloat16


def project_kernel(x_ref, wq_ref, wk_ref, wv_ref, cos_ref, sin_ref, q_ref, kv_ref):
    x = x_ref[...]
    cos = cos_ref[...]
    sin = sin_ref[...]
    lane = lax.broadcasted_iota(jnp.int32, (ROWS, WIDTH), 1)
    first = (lane & (HEAD_DIM - 1)) < HEAD_DIM // 2

    def turned(t):
        partner = jnp.where(first, pltpu.roll(t, WIDTH - HEAD_DIM // 2, 1), pltpu.roll(t, HEAD_DIM // 2, 1))
        return t * cos + partner * sin

    k = jnp.dot(x, wk_ref[...], preferred_element_type=f32)
    kv_ref[:, :WIDTH] = turned(k).astype(bf16)
    v = jnp.dot(x, wv_ref[...], preferred_element_type=f32)
    kv_ref[:, WIDTH:] = v.astype(bf16)
    q = jnp.dot(x, wq_ref[...], preferred_element_type=f32)
    q = (turned(q) * (HEAD_DIM**-0.5)).astype(bf16)
    for i in range(TEAM):
        q_ref[i] = q


def project(x, wq, wk, wv, cos, sin):
    return pl.pallas_call(
        project_kernel,
        out_shape=(
            jax.ShapeDtypeStruct((TEAM, ROWS, WIDTH), bf16),
            jax.ShapeDtypeStruct((ROWS, 2 * WIDTH), bf16),
        ),
        name="project",
    )(x, wq, wk, wv, cos, sin)


def attend_kernel(pairs_ref, count_ref, q_ref, *refs):
    kv_refs = refs[:RING]
    out_ref = refs[RING]
    qq, kbuf, vbuf, sbuf, mbuf, lbuf, acc, lse = refs[RING + 1 :]
    lane = lax.broadcasted_iota(jnp.int32, (BLK, WIDTH), 1)
    left = lane < HEAD_DIM
    for s in range(RING):
        for b in range(PER):
            rows = pl.ds(b * BLK, BLK)
            kbuf[s * PER + b] = kv_refs[s][rows, :WIDTH]
            vbuf[s * PER + b] = kv_refs[s][rows, WIDTH:]
    zero = jnp.zeros((BLK, WIDTH), bf16)
    for i in range(TEAM):
        for b in range(PER):
            q = q_ref[i, pl.ds(b * BLK, BLK), :]
            qq[i * PER + b, :BLK, :] = jnp.where(left, q, zero)
            qq[i * PER + b, BLK:, :] = jnp.where(left, zero, q)
    qq[QB] = jnp.zeros((2 * BLK, WIDTH), bf16)
    mbuf[...] = jnp.full(mbuf.shape, masked_score, f32)
    lbuf[...] = jnp.zeros(lbuf.shape, f32)
    acc[...] = jnp.zeros(acc.shape, f32)
    trips = count_ref[0]

    def score(it, carry):
        for u in range(UNROLL):
            i = it * UNROLL + u
            code = pairs_ref[i]
            qi = code >> 6
            ki = code & 63
            st = lax.dot_general(
                kbuf[ki], qq[qi], (((1,), (1,)), ((), ())), preferred_element_type=f32
            )
            sbuf[i] = st
            m8 = jnp.max(st.reshape(8, 8, WIDTH), axis=0)
            mbuf[qi] = jnp.maximum(mbuf[qi], m8)
        return carry

    lax.fori_loop(0, trips, score, 0)
    for i in range(QB + 1):
        mbuf[i] = jnp.broadcast_to(jnp.max(mbuf[i], axis=0, keepdims=True), (8, WIDTH))

    def weigh(it, carry):
        for u in range(UNROLL):
            i = it * UNROLL + u
            code = pairs_ref[i]
            qi = code >> 6
            ki = code & 63
            p = jnp.exp(sbuf[i].reshape(8, 8, WIDTH) - mbuf[qi][None])
            lbuf[qi] = lbuf[qi] + jnp.sum(p, axis=0)
            pb = p.reshape(BLK, WIDTH).astype(bf16)
            ot = lax.dot_general(
                vbuf[ki], pb, (((0,), (0,)), ((), ())), preferred_element_type=f32
            )
            acc[qi] = acc[qi] + jnp.where(left, ot[:HEAD_DIM], ot[HEAD_DIM:])
        return carry

    lax.fori_loop(0, trips, weigh, 0)
    for i in range(QB):
        total = jnp.sum(lbuf[i], axis=0, keepdims=True)
        some = total > 0.0
        safe = jnp.where(some, total, 1.0)
        out_ref[i // PER, pl.ds((i % PER) * BLK, BLK), :] = (acc[i] * (1.0 / safe)).astype(bf16)
        lse[pl.ds(i, 1), :] = jnp.where(some, mbuf[i, :1, :] + jnp.log(safe), masked_score)
    for i in range(TEAM):
        value = lse[pl.ds(i * PER, PER), :]
        hi = value.astype(bf16).astype(f32)
        rest = value - hi
        mid = rest.astype(bf16).astype(f32)
        parts = jnp.concatenate([hi, mid, rest - mid, jnp.zeros((PER, WIDTH), f32)], axis=0)
        out_ref[i, pl.ds(ROWS, STATS), :] = parts.astype(bf16)


def attend(pairs, count, q, kvs):
    smem = pl.BlockSpec(memory_space=pltpu.SMEM)
    vmem = pl.BlockSpec(memory_space=pltpu.VMEM)
    return pl.pallas_call(
        attend_kernel,
        out_shape=jax.ShapeDtypeStruct((TEAM, ROWS + STATS, WIDTH), bf16),
        in_specs=[smem, smem] + [vmem] * (1 + RING),
        out_specs=vmem,
        scratch_shapes=[
            pltpu.VMEM((QB + 1, 2 * BLK, WIDTH), bf16),
            pltpu.VMEM((RING * PER, BLK, WIDTH), bf16),
            pltpu.VMEM((RING * PER, BLK, WIDTH), bf16),
            pltpu.VMEM((MAXP, BLK, WIDTH), f32),
            pltpu.VMEM((QB + 1, 8, WIDTH), f32),
            pltpu.VMEM((QB + 1, 8, WIDTH), f32),
            pltpu.VMEM((QB + 1, BLK, WIDTH), f32),
            pltpu.VMEM((QB, WIDTH), f32),
        ],
        name="attend",
    )(pairs, count, q, *kvs)


def merge_kernel(part_ref, att_ref, log_ref):
    values = []
    for i in range(TEAM):
        st = part_ref[i, pl.ds(ROWS, STATS), :].astype(f32)
        values.append(st[:PER] + st[PER : 2 * PER] + st[2 * PER : 3 * PER])
    top = functools.reduce(jnp.maximum, values)
    weights = [jnp.exp(v - top) for v in values]
    total = functools.reduce(jnp.add, weights)
    log_ref[...] = top + jnp.log(total)
    inverse = 1.0 / total
    weights = [w * inverse for w in weights]
    for b in range(PER):
        rows = pl.ds(b * BLK, BLK)
        att = jnp.zeros((BLK, WIDTH), f32)
        for i in range(TEAM):
            att = att + part_ref[i, rows, :].astype(f32) * weights[i][b : b + 1, :]
        turned = att.T
        att_ref[rows, :] = jnp.concatenate([turned[:BLK], turned[BLK:]], axis=1).astype(bf16)


def merge(parts):
    return pl.pallas_call(
        merge_kernel,
        out_shape=(
            jax.ShapeDtypeStruct((ROWS, WIDTH), bf16),
            jax.ShapeDtypeStruct((PER, WIDTH), f32),
        ),
        name="merge",
    )(parts)


def pair_list(chosen, zh, mine):
    lists = lax.dynamic_slice_in_dim(chosen, zh * QB, QB, 0)
    here = (lists >= 0) & (((lists >> 2) & (TEAM - 1)) == mine)
    slot = (zh - (lists >> 5)) & (RING - 1)
    code = jnp.arange(QB, dtype=jnp.int32)[:, None] * 64 + slot * PER + (lists & (PER - 1))
    here = here.reshape(-1)
    code = code.reshape(-1)
    index = jnp.arange(MAXP, dtype=jnp.int32)
    before = jnp.sum(jnp.where(index[:, None] < index[None, :], here[:, None], False).astype(jnp.int32), axis=0)
    place = jnp.where(here, before, -1)
    hit = place[:, None] == index[None, :]
    pairs = jnp.sum(jnp.where(hit, code[:, None], 0), axis=0)
    count = jnp.sum(here.astype(jnp.int32))
    pairs = jnp.where(index < count, pairs, QB * 64)
    return pairs, ((count + UNROLL - 1) // UNROLL).reshape(1)


def shifted(value, step):
    return lax.ppermute(value, "zh", [(i, (i + step) % RING) for i in range(RING)])


def local(tokens, w_query, w_key, w_value, w_out, chosen):
    zh = lax.axis_index("zh")
    mine = lax.axis_index(("zl", "y"))
    device = zh * TEAM + mine
    positions = device * ROWS + jnp.arange(ROWS)
    half = HEAD_DIM // 2
    inverse = rotary_base ** (-jnp.arange(half, dtype=f32) / half)
    angles = positions.astype(f32)[:, None] * jnp.tile(inverse, 2 * WIDTH // HEAD_DIM)[None, :]
    sign = jnp.where((jnp.arange(WIDTH) & (HEAD_DIM - 1)) < half, -1.0, 1.0).astype(f32)
    q8, kv = project(
        tokens, w_query, w_key, w_value, jnp.cos(angles), jnp.sin(angles) * sign[None, :]
    )
    pairs, count = pair_list(chosen, zh, mine)
    q_team = lax.all_to_all(q8, ("zl", "y"), 0, 0, tiled=True)
    w_all = lax.all_to_all(
        jnp.broadcast_to(w_out[None], (8,) + w_out.shape), ("x", "c"), 0, 0, tiled=True
    )
    slots = [kv] + [None] * (RING - 1)
    up = down = kv
    for s in range(1, RING // 2 + 1):
        up = shifted(up, 1)
        slots[s] = up
        if s < RING // 2:
            down = shifted(down, -1)
            slots[RING - s] = down
    parts = attend(pairs, count, q_team, slots)
    parts = lax.all_to_all(parts, ("zl", "y"), 0, 0, tiled=True)
    attended, logs = merge(parts)
    log_sums = jnp.transpose(logs.reshape(PER, 2, BLK), (1, 0, 2)).reshape(2, ROWS)
    rows = lax.all_to_all(attended.reshape(8, ROWS // 8, WIDTH), ("x", "c"), 0, 0, tiled=True)
    output = jnp.einsum("trc,tcn->rn", rows, w_all, preferred_element_type=f32)
    return (output.astype(bf16), log_sums)


def solution(mesh):
    fine = Mesh(mesh.devices.reshape(8, 2, 4, 4, 2), ("zh", "zl", "y", "x", "c"))
    kv = ("zh", "zl", "y")
    tp = ("x", "c")
    placed = (P(kv, None), P(None, tp), P(None, tp), P(None, tp), P(tp, None), P())
    return jax.shard_map(
        local,
        mesh=fine,
        in_specs=placed,
        out_specs=(P(kv + tp, None), P(tp, kv)),
        check_vma=False,
    )
```

```python
import functools

import jax
import jax.numpy as jnp
from jax import lax
from jax.experimental import pallas as pl
from jax.experimental.pallas import tpu as pltpu
from jax.sharding import Mesh
from jax.sharding import PartitionSpec as P

HEAD_DIM = 64
BLK = 64
SEL = 16
ROWS = 256
PER = 4
WIDTH = 128
RING = 8
TEAM = 8
QB = TEAM * PER
MAXP = QB * SEL
UNROLL = 8
STATS = 16

rotary_base = 500000.0
masked_score = -1e30
f32 = jnp.float32
bf16 = jnp.bfloat16


def project_kernel(x_ref, wq_ref, wk_ref, wv_ref, cos_ref, sin_ref, q_ref, kv_ref):
    x = x_ref[...]
    cos = cos_ref[...]
    sin = sin_ref[...]
    lane = lax.broadcasted_iota(jnp.int32, (ROWS, WIDTH), 1)
    first = (lane & (HEAD_DIM - 1)) < HEAD_DIM // 2

    def turned(t):
        partner = jnp.where(first, pltpu.roll(t, WIDTH - HEAD_DIM // 2, 1), pltpu.roll(t, HEAD_DIM // 2, 1))
        return t * cos + partner * sin

    k = jnp.dot(x, wk_ref[...], preferred_element_type=f32)
    kv_ref[:, :WIDTH] = turned(k).astype(bf16)
    v = jnp.dot(x, wv_ref[...], preferred_element_type=f32)
    kv_ref[:, WIDTH:] = v.astype(bf16)
    q = jnp.dot(x, wq_ref[...], preferred_element_type=f32)
    q = (turned(q) * (HEAD_DIM**-0.5)).astype(bf16)
    for i in range(TEAM):
        q_ref[i] = q


def project(x, wq, wk, wv, cos, sin):
    return pl.pallas_call(
        project_kernel,
        out_shape=(
            jax.ShapeDtypeStruct((TEAM, ROWS, WIDTH), bf16),
            jax.ShapeDtypeStruct((ROWS, 2 * WIDTH), bf16),
        ),
        compiler_params=pltpu.CompilerParams(vmem_limit_bytes=12 << 20),
        name="project",
    )(x, wq, wk, wv, cos, sin)


def attend_kernel(pairs_ref, count_ref, q_ref, *refs):
    kv_refs = refs[:RING]
    out_ref = refs[RING]
    qq, kbuf, vbuf, sbuf, mbuf, lbuf, acc, lse = refs[RING + 1 :]
    lane = lax.broadcasted_iota(jnp.int32, (BLK, WIDTH), 1)
    left = lane < HEAD_DIM
    for s in range(RING):
        for b in range(PER):
            rows = pl.ds(b * BLK, BLK)
            kbuf[s * PER + b] = kv_refs[s][rows, :WIDTH]
            vbuf[s * PER + b] = kv_refs[s][rows, WIDTH:]
    zero = jnp.zeros((BLK, WIDTH), bf16)
    for i in range(TEAM):
        for b in range(PER):
            q = q_ref[i, pl.ds(b * BLK, BLK), :]
            qq[i * PER + b, :BLK, :] = jnp.where(left, q, zero)
            qq[i * PER + b, BLK:, :] = jnp.where(left, zero, q)
    qq[QB] = jnp.zeros((2 * BLK, WIDTH), bf16)
    mbuf[...] = jnp.full(mbuf.shape, masked_score, f32)
    lbuf[...] = jnp.zeros(lbuf.shape, f32)
    acc[...] = jnp.zeros(acc.shape, f32)
    trips = count_ref[0]

    def score(it, carry):
        for u in range(UNROLL):
            i = it * UNROLL + u
            code = pairs_ref[i]
            qi = code >> 6
            ki = code & 63
            st = lax.dot_general(
                kbuf[ki], qq[qi], (((1,), (1,)), ((), ())), preferred_element_type=f32
            )
            sbuf[i] = st
            m8 = jnp.max(st.reshape(8, 8, WIDTH), axis=0)
            mbuf[qi] = jnp.maximum(mbuf[qi], m8)
        return carry

    lax.fori_loop(0, trips, score, 0)
    for i in range(QB + 1):
        mbuf[i] = jnp.broadcast_to(jnp.max(mbuf[i], axis=0, keepdims=True), (8, WIDTH))

    def weigh(it, carry):
        for u in range(UNROLL):
            i = it * UNROLL + u
            code = pairs_ref[i]
            qi = code >> 6
            ki = code & 63
            p = jnp.exp(sbuf[i].reshape(8, 8, WIDTH) - mbuf[qi][None])
            lbuf[qi] = lbuf[qi] + jnp.sum(p, axis=0)
            pb = p.reshape(BLK, WIDTH).astype(bf16)
            ot = lax.dot_general(
                vbuf[ki], pb, (((0,), (0,)), ((), ())), preferred_element_type=f32
            )
            acc[qi] = acc[qi] + jnp.where(left, ot[:HEAD_DIM], ot[HEAD_DIM:])
        return carry

    lax.fori_loop(0, trips, weigh, 0)
    for i in range(QB):
        total = jnp.sum(lbuf[i], axis=0, keepdims=True)
        some = total > 0.0
        safe = jnp.where(some, total, 1.0)
        out_ref[i // PER, pl.ds((i % PER) * BLK, BLK), :] = (acc[i] * (1.0 / safe)).astype(bf16)
        lse[pl.ds(i, 1), :] = jnp.where(some, mbuf[i, :1, :] + jnp.log(safe), masked_score)
    for i in range(TEAM):
        value = lse[pl.ds(i * PER, PER), :]
        hi = value.astype(bf16).astype(f32)
        rest = value - hi
        mid = rest.astype(bf16).astype(f32)
        parts = jnp.concatenate([hi, mid, rest - mid, jnp.zeros((PER, WIDTH), f32)], axis=0)
        out_ref[i, pl.ds(ROWS, STATS), :] = parts.astype(bf16)


def attend(pairs, count, q, kvs):
    smem = pl.BlockSpec(memory_space=pltpu.SMEM)
    vmem = pl.BlockSpec(memory_space=pltpu.VMEM)
    return pl.pallas_call(
        attend_kernel,
        out_shape=jax.ShapeDtypeStruct((TEAM, ROWS + STATS, WIDTH), bf16),
        in_specs=[smem, smem] + [vmem] * (1 + RING),
        out_specs=vmem,
        scratch_shapes=[
            pltpu.VMEM((QB + 1, 2 * BLK, WIDTH), bf16),
            pltpu.VMEM((RING * PER, BLK, WIDTH), bf16),
            pltpu.VMEM((RING * PER, BLK, WIDTH), bf16),
            pltpu.VMEM((MAXP, BLK, WIDTH), f32),
            pltpu.VMEM((QB + 1, 8, WIDTH), f32),
            pltpu.VMEM((QB + 1, 8, WIDTH), f32),
            pltpu.VMEM((QB + 1, BLK, WIDTH), f32),
            pltpu.VMEM((QB, WIDTH), f32),
        ],
        compiler_params=pltpu.CompilerParams(vmem_limit_bytes=28 << 20),
        name="attend",
    )(pairs, count, q, *kvs)


def merge_kernel(part_ref, att_ref, log_ref):
    values = []
    for i in range(TEAM):
        st = part_ref[i, pl.ds(ROWS, STATS), :].astype(f32)
        values.append(st[:PER] + st[PER : 2 * PER] + st[2 * PER : 3 * PER])
    top = functools.reduce(jnp.maximum, values)
    weights = [jnp.exp(v - top) for v in values]
    total = functools.reduce(jnp.add, weights)
    log_ref[...] = top + jnp.log(total)
    inverse = 1.0 / total
    weights = [w * inverse for w in weights]
    for b in range(PER):
        rows = pl.ds(b * BLK, BLK)
        att = jnp.zeros((BLK, WIDTH), f32)
        for i in range(TEAM):
            att = att + part_ref[i, rows, :].astype(f32) * weights[i][b : b + 1, :]
        turned = att.T
        att_ref[rows, :] = jnp.concatenate([turned[:BLK], turned[BLK:]], axis=1).astype(bf16)


def merge(parts):
    return pl.pallas_call(
        merge_kernel,
        out_shape=(
            jax.ShapeDtypeStruct((ROWS, WIDTH), bf16),
            jax.ShapeDtypeStruct((PER, WIDTH), f32),
        ),
        compiler_params=pltpu.CompilerParams(vmem_limit_bytes=4 << 20),
        name="merge",
    )(parts)


def pair_list(chosen, zh, mine):
    lists = lax.dynamic_slice_in_dim(chosen, zh * QB, QB, 0)
    here = (lists >= 0) & (((lists >> 2) & (TEAM - 1)) == mine)
    slot = (zh - (lists >> 5)) & (RING - 1)
    code = jnp.arange(QB, dtype=jnp.int32)[:, None] * 64 + slot * PER + (lists & (PER - 1))
    here = here.reshape(-1)
    code = code.reshape(-1)
    index = jnp.arange(MAXP, dtype=jnp.int32)
    before = jnp.sum(jnp.where(index[:, None] < index[None, :], here[:, None], False).astype(jnp.int32), axis=0)
    place = jnp.where(here, before, -1)
    hit = place[:, None] == index[None, :]
    pairs = jnp.sum(jnp.where(hit, code[:, None], 0), axis=0)
    count = jnp.sum(here.astype(jnp.int32))
    pairs = jnp.where(index < count, pairs, QB * 64)
    return pairs, ((count + UNROLL - 1) // UNROLL).reshape(1)


def up_pairs(step):
    return [(i, i + 1) for i in range(step - 1, RING - 1)]


def down_pairs(step):
    far = RING // 2 - 1
    return [((r - step + 1) % RING, (r - step) % RING) for r in range(far)]


def local(tokens, w_query, w_key, w_value, w_out, chosen):
    zh = lax.axis_index("zh")
    mine = lax.axis_index(("zl", "y"))
    device = zh * TEAM + mine
    positions = device * ROWS + jnp.arange(ROWS)
    half = HEAD_DIM // 2
    inverse = rotary_base ** (-jnp.arange(half, dtype=f32) / half)
    angles = positions.astype(f32)[:, None] * jnp.tile(inverse, 2 * WIDTH // HEAD_DIM)[None, :]
    sign = jnp.where((jnp.arange(WIDTH) & (HEAD_DIM - 1)) < half, -1.0, 1.0).astype(f32)
    q8, kv = project(
        tokens, w_query, w_key, w_value, jnp.cos(angles), jnp.sin(angles) * sign[None, :]
    )
    pairs, count = pair_list(chosen, zh, mine)
    slots = [kv] + [None] * (RING - 1)
    up = down = kv
    for s in range(1, RING // 2 + 1):
        up = lax.ppermute(up, "zh", up_pairs(s))
        slots[s] = up
        if s < RING // 2:
            down = lax.ppermute(down, "zh", down_pairs(s))
            slots[RING - s] = down
    q_team = lax.all_to_all(q8, ("zl", "y"), 0, 0, tiled=True)
    w_same = lax.all_to_all(
        jnp.broadcast_to(w_out[None], (4,) + w_out.shape), "x", 0, 0, tiled=True
    )
    w_other = lax.ppermute(w_same, "c", [(0, 1), (1, 0)])
    parts = attend(pairs, count, q_team, slots)
    parts = lax.all_to_all(parts, ("zl", "y"), 0, 0, tiled=True)
    attended, logs = merge(parts)
    log_sums = jnp.transpose(logs.reshape(PER, 2, BLK), (1, 0, 2)).reshape(2, ROWS)
    rows = lax.all_to_all(attended.reshape(8, ROWS // 8, WIDTH), ("x", "c"), 0, 0, tiled=True)
    rows = rows.reshape(4, 2, ROWS // 8, WIDTH)
    core = lax.axis_index("c")
    rows_same = lax.dynamic_index_in_dim(rows, core, 1, keepdims=False)
    rows_other = lax.dynamic_index_in_dim(rows, 1 - core, 1, keepdims=False)
    output = jnp.einsum("trc,tcn->rn", rows_same, w_same, preferred_element_type=f32)
    output = output + jnp.einsum("trc,tcn->rn", rows_other, w_other, preferred_element_type=f32)
    return (output.astype(bf16), log_sums)


def solution(mesh):
    fine = Mesh(mesh.devices.reshape(8, 2, 4, 4, 2), ("zh", "zl", "y", "x", "c"))
    kv = ("zh", "zl", "y")
    tp = ("x", "c")
    placed = (P(kv, None), P(None, tp), P(None, tp), P(None, tp), P(tp, None), P())
    return jax.shard_map(
        local,
        mesh=fine,
        in_specs=placed,
        out_specs=(P(kv + tp, None), P(tp, kv)),
        check_vma=False,
    )
```

```python
import functools

import jax
import jax.numpy as jnp
from jax import lax
from jax.experimental import pallas as pl
from jax.experimental.pallas import tpu as pltpu
from jax.sharding import Mesh
from jax.sharding import PartitionSpec as P

HEAD_DIM = 64
BLK = 64
SEL = 16
ROWS = 256
PER = 4
WIDTH = 128
RING = 8
TEAM = 8
QB = TEAM * PER
MAXP = QB * SEL
UNROLL = 8
STATS = 16

rotary_base = 500000.0
masked_score = -1e30
f32 = jnp.float32
bf16 = jnp.bfloat16


def project_kernel(x_hbm, wq_hbm, wk_hbm, wv_hbm, cos_ref, sin_ref, q_ref, kv_ref, x_buf, w_buf, sems):
    copies = [pltpu.make_async_copy(x_hbm, x_buf, sems.at[0])]
    for i, w in enumerate((wk_hbm, wv_hbm, wq_hbm)):
        copies.append(pltpu.make_async_copy(w, w_buf.at[i], sems.at[i + 1]))
    for copy in copies:
        copy.start()
    cos = cos_ref[...]
    sin = sin_ref[...]
    lane = lax.broadcasted_iota(jnp.int32, (ROWS, WIDTH), 1)
    first = (lane & (HEAD_DIM - 1)) < HEAD_DIM // 2

    def turned(t):
        partner = jnp.where(first, pltpu.roll(t, WIDTH - HEAD_DIM // 2, 1), pltpu.roll(t, HEAD_DIM // 2, 1))
        return t * cos + partner * sin

    copies[0].wait()
    copies[1].wait()
    x = x_buf[...]
    k = jnp.dot(x, w_buf[0], preferred_element_type=f32)
    kv_ref[:, :WIDTH] = turned(k).astype(bf16)
    copies[2].wait()
    v = jnp.dot(x, w_buf[1], preferred_element_type=f32)
    kv_ref[:, WIDTH:] = v.astype(bf16)
    copies[3].wait()
    q = jnp.dot(x, w_buf[2], preferred_element_type=f32)
    q = (turned(q) * (HEAD_DIM**-0.5)).astype(bf16)
    for i in range(TEAM):
        q_ref[i] = q


def project(x, wq, wk, wv, cos, sin):
    hbm = pl.BlockSpec(memory_space=pltpu.HBM)
    vmem = pl.BlockSpec(memory_space=pltpu.VMEM)
    return pl.pallas_call(
        project_kernel,
        out_shape=(
            jax.ShapeDtypeStruct((TEAM, ROWS, WIDTH), bf16),
            jax.ShapeDtypeStruct((ROWS, 2 * WIDTH), bf16),
        ),
        in_specs=[hbm] * 4 + [vmem] * 2,
        out_specs=(vmem, vmem),
        scratch_shapes=[
            pltpu.VMEM(x.shape, bf16),
            pltpu.VMEM((3,) + wq.shape, bf16),
            pltpu.SemaphoreType.DMA((4,)),
        ],
        name="project",
    )(x, wq, wk, wv, cos, sin)


def attend_kernel(pairs_ref, count_ref, q_ref, *refs):
    kv_refs = refs[:RING]
    out_ref = refs[RING]
    qq, kbuf, vbuf, sbuf, mbuf, lbuf, acc = refs[RING + 1 :]
    lane = lax.broadcasted_iota(jnp.int32, (BLK, WIDTH), 1)
    left = lane < HEAD_DIM
    even = (lane & (HEAD_DIM // 2)) == 0
    for s in range(RING):
        for b in range(PER):
            rows = pl.ds(b * BLK, BLK)
            kbuf[s * PER + b] = kv_refs[s][rows, :WIDTH]
            vbuf[s * PER + b] = kv_refs[s][rows, WIDTH:]
    half = BLK // 2
    left_half = left[:half]
    zero = jnp.zeros((half, WIDTH), bf16)
    for i in range(TEAM):
        for b in range(PER):
            for h in range(2):
                q = q_ref[i, pl.ds(b * BLK + h * half, half), :]
                qq[i * PER + b, pl.ds(h * BLK, half), :] = jnp.where(left_half, q, zero)
                qq[i * PER + b, pl.ds(h * BLK + half, half), :] = jnp.where(left_half, zero, q)
    qq[QB] = jnp.zeros((2 * BLK, WIDTH), bf16)
    mbuf[...] = jnp.full(mbuf.shape, masked_score, f32)
    lbuf[...] = jnp.zeros(lbuf.shape, f32)
    acc[...] = jnp.zeros(acc.shape, f32)
    trips = count_ref[0]

    def score(it, carry):
        for u in range(UNROLL):
            i = it * UNROLL + u
            code = pairs_ref[i]
            qi = code >> 6
            ki = code & 63
            st = lax.dot_general(
                kbuf[ki], qq[qi], (((1,), (1,)), ((), ())), preferred_element_type=f32
            )
            sbuf[i] = st
            m8 = jnp.max(st.reshape(8, 8, WIDTH), axis=0)
            mbuf[qi] = jnp.maximum(mbuf[qi], m8)
        return carry

    lax.fori_loop(0, trips, score, 0)
    for i in range(QB + 1):
        mbuf[i] = jnp.broadcast_to(jnp.max(mbuf[i], axis=0, keepdims=True), (8, WIDTH))

    def weigh(it, carry):
        for u in range(UNROLL):
            i = it * UNROLL + u
            code = pairs_ref[i]
            qi = code >> 6
            ki = code & 63
            p = jnp.exp(sbuf[i].reshape(8, 8, WIDTH) - mbuf[qi][None])
            lbuf[qi] = lbuf[qi] + jnp.sum(p, axis=0)
            pb = p.reshape(BLK, WIDTH).astype(bf16)
            ot = lax.dot_general(
                vbuf[ki], pb, (((0,), (0,)), ((), ())), preferred_element_type=f32
            )
            acc[qi] = acc[qi] + jnp.where(even, ot[:HEAD_DIM], ot[HEAD_DIM:])
        return carry

    lax.fori_loop(0, trips, weigh, 0)
    left_row = left[:1]

    def finished(i):
        total = jnp.sum(lbuf[i], axis=0, keepdims=True)
        some = total > 0.0
        safe = jnp.where(some, total, 1.0)
        return acc[i] * (1.0 / safe), jnp.where(some, mbuf[i, :1, :] + jnp.log(safe), masked_score)

    for i in range(TEAM):
        logs = []
        for pair in range(PER // 2):
            one, one_log = finished(i * PER + 2 * pair)
            two, two_log = finished(i * PER + 2 * pair + 1)
            rows = pl.ds(pair * BLK, BLK)
            out_ref[2 * i, rows, :] = jnp.where(left, one, pltpu.roll(two, BLK, 1)).astype(bf16)
            out_ref[2 * i + 1, rows, :] = jnp.where(left, pltpu.roll(one, BLK, 1), two).astype(bf16)
            logs.append(
                (
                    jnp.where(left_row, one_log, pltpu.roll(two_log, BLK, 1)),
                    jnp.where(left_row, pltpu.roll(one_log, BLK, 1), two_log),
                )
            )
        for c in range(2):
            value = jnp.concatenate([logs[0][c], logs[1][c]], axis=0)
            hi = value.astype(bf16).astype(f32)
            rest = value - hi
            mid = rest.astype(bf16).astype(f32)
            empty = jnp.zeros((STATS - 6, WIDTH), f32)
            stats = jnp.concatenate([hi, mid, rest - mid, empty], axis=0)
            out_ref[2 * i + c, pl.ds(2 * BLK, STATS), :] = stats.astype(bf16)


def attend(pairs, count, q, kvs):
    smem = pl.BlockSpec(memory_space=pltpu.SMEM)
    vmem = pl.BlockSpec(memory_space=pltpu.VMEM)
    return pl.pallas_call(
        attend_kernel,
        out_shape=jax.ShapeDtypeStruct((2 * TEAM, 2 * BLK + STATS, WIDTH), bf16),
        in_specs=[smem, smem] + [vmem] * (1 + RING),
        out_specs=vmem,
        scratch_shapes=[
            pltpu.VMEM((QB + 1, 2 * BLK, WIDTH), bf16),
            pltpu.VMEM((RING * PER, BLK, WIDTH), bf16),
            pltpu.VMEM((RING * PER, BLK, WIDTH), bf16),
            pltpu.VMEM((MAXP, BLK, WIDTH), f32),
            pltpu.VMEM((QB + 1, 8, WIDTH), f32),
            pltpu.VMEM((QB + 1, 8, WIDTH), f32),
            pltpu.VMEM((QB + 1, BLK, WIDTH), f32),
        ],
        compiler_params=pltpu.CompilerParams(vmem_limit_bytes=28 << 20),
        name="attend",
    )(pairs, count, q, *kvs)


def merge_kernel(core_ref, part_ref, same_ref, other_ref, out_ref, log_ref, att):
    half = BLK // 2
    for c in range(2):
        values = []
        for i in range(TEAM):
            st = part_ref[2 * i + c, pl.ds(2 * BLK, STATS), :].astype(f32)
            values.append(st[:2] + st[2:4] + st[4:6])
        top = functools.reduce(jnp.maximum, values)
        weights = [jnp.exp(v - top) for v in values]
        total = functools.reduce(jnp.add, weights)
        log_ref[pl.ds(2 * c, 2), :] = top + jnp.log(total)
        inverse = 1.0 / total
        weights = [w * inverse for w in weights]
        for pair in range(PER // 2):
            mixed = jnp.zeros((BLK, WIDTH), f32)
            for i in range(TEAM):
                part = part_ref[2 * i + c, pl.ds(pair * BLK, BLK), :].astype(f32)
                mixed = mixed + part * weights[i][pair : pair + 1, :]
            turned = mixed.T
            for b in range(2):
                heads = [turned[b * BLK + h * half : b * BLK + (h + 1) * half] for h in range(2)]
                rows = pl.ds((2 * pair + b) * half, half)
                att[c, rows, :] = jnp.concatenate(heads, axis=1).astype(bf16)
    core = core_ref[0]
    y = jnp.dot(att[core], same_ref[...], preferred_element_type=f32)
    y = y + jnp.dot(att[1 - core], other_ref[...], preferred_element_type=f32)
    out_ref[...] = y.astype(bf16).reshape(out_ref.shape)


def merge(core, parts, w_same, w_other):
    smem = pl.BlockSpec(memory_space=pltpu.SMEM)
    vmem = pl.BlockSpec(memory_space=pltpu.VMEM)
    return pl.pallas_call(
        merge_kernel,
        out_shape=(
            jax.ShapeDtypeStruct((PER, BLK // 2, w_same.shape[1]), bf16),
            jax.ShapeDtypeStruct((4, WIDTH), f32),
        ),
        in_specs=[smem, vmem, vmem, vmem],
        out_specs=(vmem, vmem),
        scratch_shapes=[pltpu.VMEM((2, 2 * BLK, WIDTH), bf16)],
        compiler_params=pltpu.CompilerParams(vmem_limit_bytes=12 << 20),
        name="merge",
    )(core.reshape(1), parts, w_same, w_other)


def pair_list(chosen, zh, mine):
    lists = lax.dynamic_slice_in_dim(chosen, zh * QB, QB, 0)
    here = (lists >= 0) & (((lists >> 2) & (TEAM - 1)) == mine)
    slot = (zh - (lists >> 5)) & (RING - 1)
    code = jnp.arange(QB, dtype=jnp.int32)[:, None] * 64 + slot * PER + (lists & (PER - 1))
    here = here.reshape(-1)
    code = code.reshape(-1)
    index = jnp.arange(MAXP, dtype=jnp.int32)
    before = jnp.sum(jnp.where(index[:, None] < index[None, :], here[:, None], False).astype(jnp.int32), axis=0)
    place = jnp.where(here, before, -1)
    hit = place[:, None] == index[None, :]
    pairs = jnp.sum(jnp.where(hit, code[:, None], 0), axis=0)
    count = jnp.sum(here.astype(jnp.int32))
    pairs = jnp.where(index < count, pairs, QB * 64)
    return pairs, ((count + UNROLL - 1) // UNROLL).reshape(1)


def up_pairs(step):
    return [(i, i + 1) for i in range(step - 1, RING - 1)]


def down_pairs(step):
    far = RING // 2 - 1
    return [((r - step + 1) % RING, (r - step) % RING) for r in range(far)]


def local(tokens, w_query, w_key, w_value, w_out, chosen):
    zh = lax.axis_index("zh")
    mine = lax.axis_index(("zl", "y"))
    device = zh * TEAM + mine
    positions = device * ROWS + jnp.arange(ROWS)
    half = HEAD_DIM // 2
    inverse = rotary_base ** (-jnp.arange(half, dtype=f32) / half)
    angles = positions.astype(f32)[:, None] * jnp.tile(inverse, 2 * WIDTH // HEAD_DIM)[None, :]
    sign = jnp.where((jnp.arange(WIDTH) & (HEAD_DIM - 1)) < half, -1.0, 1.0).astype(f32)
    q8, kv = project(
        tokens, w_query, w_key, w_value, jnp.cos(angles), jnp.sin(angles) * sign[None, :]
    )
    pairs, count = pair_list(chosen, zh, mine)
    slots = [kv] + [None] * (RING - 1)
    up = down = kv
    for s in range(1, RING // 2 + 1):
        up = lax.ppermute(up, "zh", up_pairs(s))
        slots[s] = up
        if s < RING // 2:
            down = lax.ppermute(down, "zh", down_pairs(s))
            slots[RING - s] = down
    q_team = lax.all_to_all(q8, ("zl", "y"), 0, 0, tiled=True)
    core = lax.axis_index("c")
    w_other = lax.ppermute(w_out, "c", [(0, 1), (1, 0)])
    parts = attend(pairs, count, q_team, slots)
    parts = lax.all_to_all(parts, ("zl", "y", "c"), 0, 0, tiled=True)
    partial, logs = merge(core, parts, w_out, w_other)
    tiles = lax.all_to_all(partial, "x", 0, 0, tiled=True)
    logs = logs.reshape(2, 2, 2, 2, BLK // 2)
    mine_logs = lax.dynamic_index_in_dim(logs, core, 0, keepdims=False)
    other_logs = lax.ppermute(
        lax.dynamic_index_in_dim(logs, 1 - core, 0, keepdims=False), "c", [(0, 1), (1, 0)]
    )
    ordered = jnp.where(
        core == 0, jnp.stack([mine_logs, other_logs]), jnp.stack([other_logs, mine_logs])
    )
    log_sums = jnp.transpose(ordered, (3, 1, 2, 0, 4)).reshape(2, ROWS)
    output = jnp.sum(tiles.astype(f32), axis=0)
    return (output.astype(bf16), log_sums)


def solution(mesh):
    fine = Mesh(mesh.devices.reshape(8, 2, 4, 4, 2), ("zh", "zl", "y", "x", "c"))
    kv = ("zh", "zl", "y")
    tp = ("x", "c")
    placed = (P(kv, None), P(None, tp), P(None, tp), P(None, tp), P(tp, None), P())
    return jax.shard_map(
        local,
        mesh=fine,
        in_specs=placed,
        out_specs=(P(kv + tp, None), P(tp, kv)),
        check_vma=False,
    )
```

```python
import functools

import jax
import jax.numpy as jnp
from jax import lax
from jax.experimental import pallas as pl
from jax.experimental.pallas import tpu as pltpu
from jax.sharding import Mesh
from jax.sharding import PartitionSpec as P

HEAD_DIM = 64
BLK = 64
SEL = 16
ROWS = 256
PER = 4
WIDTH = 128
RING = 8
TEAM = 8
QB = TEAM * PER
MAXP = QB * SEL
UNROLL = 8
NEAR = (0, 1, 2, 6, 7)
FAR = (3, 4, 5)
STATS = 16

rotary_base = 500000.0
masked_score = -1e30
f32 = jnp.float32
bf16 = jnp.bfloat16


def project_kernel(x_hbm, wq_hbm, wk_hbm, wv_hbm, cos_ref, sin_ref, q_ref, kv_ref, x_buf, w_buf, sems):
    copies = [pltpu.make_async_copy(x_hbm, x_buf, sems.at[0])]
    for i, w in enumerate((wk_hbm, wv_hbm, wq_hbm)):
        copies.append(pltpu.make_async_copy(w, w_buf.at[i], sems.at[i + 1]))
    for copy in copies:
        copy.start()
    cos = cos_ref[...]
    sin = sin_ref[...]
    lane = lax.broadcasted_iota(jnp.int32, (ROWS, WIDTH), 1)
    first = (lane & (HEAD_DIM - 1)) < HEAD_DIM // 2

    def turned(t):
        partner = jnp.where(first, pltpu.roll(t, WIDTH - HEAD_DIM // 2, 1), pltpu.roll(t, HEAD_DIM // 2, 1))
        return t * cos + partner * sin

    copies[0].wait()
    copies[1].wait()
    x = x_buf[...]
    k = jnp.dot(x, w_buf[0], preferred_element_type=f32)
    kv_ref[:, :WIDTH] = turned(k).astype(bf16)
    copies[2].wait()
    v = jnp.dot(x, w_buf[1], preferred_element_type=f32)
    kv_ref[:, WIDTH:] = v.astype(bf16)
    copies[3].wait()
    q = jnp.dot(x, w_buf[2], preferred_element_type=f32)
    q = (turned(q) * (HEAD_DIM**-0.5)).astype(bf16)
    for i in range(TEAM):
        q_ref[i] = q


def project(x, wq, wk, wv, cos, sin):
    x, wq, wk, wv = (pltpu.with_memory_space_constraint(a, pltpu.HBM) for a in (x, wq, wk, wv))
    hbm = pl.BlockSpec(memory_space=pltpu.HBM)
    vmem = pl.BlockSpec(memory_space=pltpu.VMEM)
    return pl.pallas_call(
        project_kernel,
        out_shape=(
            jax.ShapeDtypeStruct((TEAM, ROWS, WIDTH), bf16),
            jax.ShapeDtypeStruct((ROWS, 2 * WIDTH), bf16),
        ),
        in_specs=[hbm] * 4 + [vmem] * 2,
        out_specs=(vmem, vmem),
        scratch_shapes=[
            pltpu.VMEM(x.shape, bf16),
            pltpu.VMEM((3,) + wq.shape, bf16),
            pltpu.SemaphoreType.DMA((4,)),
        ],
        compiler_params=pltpu.CompilerParams(vmem_limit_bytes=12 << 20),
        name="project",
    )(x, wq, wk, wv, cos, sin)


def fill_keys(kv_refs, kbuf, vbuf):
    for s, ref in enumerate(kv_refs):
        for b in range(PER):
            rows = pl.ds(b * BLK, BLK)
            kbuf[s * PER + b] = ref[rows, :WIDTH]
            vbuf[s * PER + b] = ref[rows, WIDTH:]


def fill_queries(q_ref, qq):
    half = BLK // 2
    left = lax.broadcasted_iota(jnp.int32, (half, WIDTH), 1) < HEAD_DIM
    zero = jnp.zeros((half, WIDTH), bf16)
    for i in range(TEAM):
        for b in range(PER):
            for h in range(2):
                q = q_ref[i, pl.ds(b * BLK + h * half, half), :]
                qq[i * PER + b, pl.ds(h * BLK, half), :] = jnp.where(left, q, zero)
                qq[i * PER + b, pl.ds(h * BLK + half, half), :] = jnp.where(left, zero, q)
    qq[QB] = jnp.zeros((2 * BLK, WIDTH), bf16)


def run_pairs(pairs_ref, trips, qq, kbuf, vbuf, sbuf, mbuf, lbuf, acc, rescale):
    even = (lax.broadcasted_iota(jnp.int32, (BLK, WIDTH), 1) & (HEAD_DIM // 2)) == 0

    def score(it, carry):
        for u in range(UNROLL):
            i = it * UNROLL + u
            code = pairs_ref[i]
            qi = code >> 6
            ki = code & 63
            st = lax.dot_general(
                kbuf[ki], qq[qi], (((1,), (1,)), ((), ())), preferred_element_type=f32
            )
            sbuf[i] = st
            m8 = jnp.max(st.reshape(8, 8, WIDTH), axis=0)
            mbuf[qi] = jnp.maximum(mbuf[qi], m8)
        return carry

    lax.fori_loop(0, trips, score, 0)
    for i in range(QB + 1):
        top = jnp.broadcast_to(jnp.max(mbuf[i], axis=0, keepdims=True), (8, WIDTH))
        mbuf[i] = top
        if rescale is not None:
            factor = jnp.exp(rescale[i] - top)
            lbuf[i] = lbuf[i] * factor
            acc[i] = (acc[i].reshape(8, 8, WIDTH) * factor[None]).reshape(BLK, WIDTH)

    def weigh(it, carry):
        for u in range(UNROLL):
            i = it * UNROLL + u
            code = pairs_ref[i]
            qi = code >> 6
            ki = code & 63
            p = jnp.exp(sbuf[i].reshape(8, 8, WIDTH) - mbuf[qi][None])
            lbuf[qi] = lbuf[qi] + jnp.sum(p, axis=0)
            pb = p.reshape(BLK, WIDTH).astype(bf16)
            ot = lax.dot_general(
                vbuf[ki], pb, (((0,), (0,)), ((), ())), preferred_element_type=f32
            )
            acc[qi] = acc[qi] + jnp.where(even, ot[:HEAD_DIM], ot[HEAD_DIM:])
        return carry

    lax.fori_loop(0, trips, weigh, 0)


def near_kernel(pairs_ref, count_ref, q_ref, *refs):
    n = len(NEAR)
    qq, mbuf, lbuf, acc = refs[n : n + 4]
    kbuf, vbuf, sbuf = refs[n + 4 :]
    fill_keys(refs[:n], kbuf, vbuf)
    fill_queries(q_ref, qq)
    mbuf[...] = jnp.full(mbuf.shape, masked_score, f32)
    lbuf[...] = jnp.zeros(lbuf.shape, f32)
    acc[...] = jnp.zeros(acc.shape, f32)
    run_pairs(pairs_ref, count_ref[0], qq, kbuf, vbuf, sbuf, mbuf, lbuf, acc, None)


def far_kernel(pairs_ref, count_ref, qq, m_ref, l_ref, acc_ref, *refs):
    n = len(FAR)
    out_ref = refs[n]
    kbuf, vbuf, sbuf, mbuf, lbuf, acc = refs[n + 1 :]
    fill_keys(refs[:n], kbuf, vbuf)
    mbuf[...] = m_ref[...]
    lbuf[...] = l_ref[...]
    acc[...] = acc_ref[...]
    run_pairs(pairs_ref, count_ref[0], qq, kbuf, vbuf, sbuf, mbuf, lbuf, acc, m_ref)
    left = lax.broadcasted_iota(jnp.int32, (BLK, WIDTH), 1) < HEAD_DIM
    left_row = left[:1]

    def finished(i):
        total = jnp.sum(lbuf[i], axis=0, keepdims=True)
        some = total > 0.0
        safe = jnp.where(some, total, 1.0)
        return acc[i] * (1.0 / safe), jnp.where(some, mbuf[i, :1, :] + jnp.log(safe), masked_score)

    for i in range(TEAM):
        logs = []
        for pair in range(PER // 2):
            one, one_log = finished(i * PER + 2 * pair)
            two, two_log = finished(i * PER + 2 * pair + 1)
            rows = pl.ds(pair * BLK, BLK)
            out_ref[2 * i, rows, :] = jnp.where(left, one, pltpu.roll(two, BLK, 1)).astype(bf16)
            out_ref[2 * i + 1, rows, :] = jnp.where(left, pltpu.roll(one, BLK, 1), two).astype(bf16)
            logs.append(
                (
                    jnp.where(left_row, one_log, pltpu.roll(two_log, BLK, 1)),
                    jnp.where(left_row, pltpu.roll(one_log, BLK, 1), two_log),
                )
            )
        for c in range(2):
            value = jnp.concatenate([logs[0][c], logs[1][c]], axis=0)
            hi = value.astype(bf16).astype(f32)
            rest = value - hi
            mid = rest.astype(bf16).astype(f32)
            empty = jnp.zeros((STATS - 6, WIDTH), f32)
            stats = jnp.concatenate([hi, mid, rest - mid, empty], axis=0)
            out_ref[2 * i + c, pl.ds(2 * BLK, STATS), :] = stats.astype(bf16)


STATE = (
    jax.ShapeDtypeStruct((QB + 1, 2 * BLK, WIDTH), bf16),
    jax.ShapeDtypeStruct((QB + 1, 8, WIDTH), f32),
    jax.ShapeDtypeStruct((QB + 1, 8, WIDTH), f32),
    jax.ShapeDtypeStruct((QB + 1, BLK, WIDTH), f32),
)


def key_scratch(n):
    return [
        pltpu.VMEM((n * PER, BLK, WIDTH), bf16),
        pltpu.VMEM((n * PER, BLK, WIDTH), bf16),
        pltpu.VMEM((MAXP, BLK, WIDTH), f32),
    ]


def attend_near(pairs, count, q, kvs):
    smem = pl.BlockSpec(memory_space=pltpu.SMEM)
    vmem = pl.BlockSpec(memory_space=pltpu.VMEM)
    return pl.pallas_call(
        near_kernel,
        out_shape=STATE,
        in_specs=[smem, smem] + [vmem] * (1 + len(kvs)),
        out_specs=(vmem,) * len(STATE),
        scratch_shapes=key_scratch(len(kvs)),
        compiler_params=pltpu.CompilerParams(vmem_limit_bytes=26 << 20),
        name="near",
    )(pairs, count, q, *kvs)


def attend_far(pairs, count, state, kvs):
    smem = pl.BlockSpec(memory_space=pltpu.SMEM)
    vmem = pl.BlockSpec(memory_space=pltpu.VMEM)
    return pl.pallas_call(
        far_kernel,
        out_shape=jax.ShapeDtypeStruct((2 * TEAM, 2 * BLK + STATS, WIDTH), bf16),
        in_specs=[smem, smem] + [vmem] * (len(state) + len(kvs)),
        out_specs=vmem,
        scratch_shapes=key_scratch(len(kvs)) + [pltpu.VMEM(s.shape, s.dtype) for s in STATE[1:]],
        compiler_params=pltpu.CompilerParams(vmem_limit_bytes=26 << 20),
        name="far",
    )(pairs, count, *state, *kvs)


def merge_kernel(core_ref, part_ref, same_ref, other_ref, out_ref, log_ref, att):
    half = BLK // 2
    for c in range(2):
        values = []
        for i in range(TEAM):
            st = part_ref[2 * i + c, pl.ds(2 * BLK, STATS), :].astype(f32)
            values.append(st[:2] + st[2:4] + st[4:6])
        top = functools.reduce(jnp.maximum, values)
        weights = [jnp.exp(v - top) for v in values]
        total = functools.reduce(jnp.add, weights)
        log_ref[pl.ds(2 * c, 2), :] = top + jnp.log(total)
        inverse = 1.0 / total
        weights = [w * inverse for w in weights]
        for pair in range(PER // 2):
            mixed = jnp.zeros((BLK, WIDTH), f32)
            for i in range(TEAM):
                part = part_ref[2 * i + c, pl.ds(pair * BLK, BLK), :].astype(f32)
                mixed = mixed + part * weights[i][pair : pair + 1, :]
            turned = mixed.T
            for b in range(2):
                heads = [turned[b * BLK + h * half : b * BLK + (h + 1) * half] for h in range(2)]
                rows = pl.ds((2 * pair + b) * half, half)
                att[c, rows, :] = jnp.concatenate(heads, axis=1).astype(bf16)
    core = core_ref[0]
    y = jnp.dot(att[core], same_ref[...], preferred_element_type=f32)
    y = y + jnp.dot(att[1 - core], other_ref[...], preferred_element_type=f32)
    out_ref[...] = y.astype(bf16).reshape(out_ref.shape)


def merge(core, parts, w_same, w_other):
    smem = pl.BlockSpec(memory_space=pltpu.SMEM)
    vmem = pl.BlockSpec(memory_space=pltpu.VMEM)
    return pl.pallas_call(
        merge_kernel,
        out_shape=(
            jax.ShapeDtypeStruct((PER, BLK // 2, w_same.shape[1]), bf16),
            jax.ShapeDtypeStruct((4, WIDTH), f32),
        ),
        in_specs=[smem, vmem, vmem, vmem],
        out_specs=(vmem, vmem),
        scratch_shapes=[pltpu.VMEM((2, 2 * BLK, WIDTH), bf16)],
        compiler_params=pltpu.CompilerParams(vmem_limit_bytes=12 << 20),
        name="merge",
    )(core.reshape(1), parts, w_same, w_other)


def pair_lists(chosen, zh, mine):
    lists = lax.dynamic_slice_in_dim(chosen, zh * QB, QB, 0)
    here = (lists >= 0) & (((lists >> 2) & (TEAM - 1)) == mine)
    slot = (zh - (lists >> 5)) & (RING - 1)
    far = (slot >= FAR[0]) & (slot <= FAR[-1])
    order = jnp.where(far, slot - FAR[0], jnp.where(slot > FAR[-1], slot - len(FAR), slot))
    code = jnp.arange(QB, dtype=jnp.int32)[:, None] * 64 + order * PER + (lists & (PER - 1))
    kind = jnp.where(here, jnp.where(far, 1, 0), -1).reshape(-1)
    code = code.reshape(-1)
    index = jnp.arange(MAXP, dtype=jnp.int32)
    same = kind[:, None] == kind[None, :]
    before = jnp.sum((same & (index[:, None] < index[None, :])).astype(jnp.int32), axis=0)
    out = []
    for k in range(2):
        place = jnp.where(kind == k, before, -1)
        pairs = jnp.sum(jnp.where(place[:, None] == index[None, :], code[:, None], 0), axis=0)
        count = jnp.sum((kind == k).astype(jnp.int32))
        pairs = jnp.where(index < count, pairs, QB * 64)
        out.append((pairs, ((count + UNROLL - 1) // UNROLL).reshape(1)))
    return out


def up_pairs(step):
    return [(i, i + 1) for i in range(step - 1, RING - 1)]


def down_pairs(step):
    far = RING // 2 - 1
    return [((r - step + 1) % RING, (r - step) % RING) for r in range(far)]


def local(tokens, w_query, w_key, w_value, w_out, chosen):
    zh = lax.axis_index("zh")
    mine = lax.axis_index(("zl", "y"))
    device = zh * TEAM + mine
    positions = device * ROWS + jnp.arange(ROWS)
    half = HEAD_DIM // 2
    inverse = rotary_base ** (-jnp.arange(half, dtype=f32) / half)
    angles = positions.astype(f32)[:, None] * jnp.tile(inverse, 2 * WIDTH // HEAD_DIM)[None, :]
    sign = jnp.where((jnp.arange(WIDTH) & (HEAD_DIM - 1)) < half, -1.0, 1.0).astype(f32)
    q8, kv = project(
        tokens, w_query, w_key, w_value, jnp.cos(angles), jnp.sin(angles) * sign[None, :]
    )
    near, far = pair_lists(chosen, zh, mine)
    slots = [kv] + [None] * (RING - 1)
    up = down = kv
    for s in range(1, RING // 2 + 1):
        up = lax.ppermute(up, "zh", up_pairs(s))
        slots[s] = up
        if s < RING // 2:
            down = lax.ppermute(down, "zh", down_pairs(s))
            slots[RING - s] = down
    q_team = lax.all_to_all(q8, ("zl", "y"), 0, 0, tiled=True)
    core = lax.axis_index("c")
    w_other = lax.ppermute(w_out, "c", [(0, 1), (1, 0)])
    state = attend_near(*near, q_team, [slots[i] for i in NEAR])
    parts = attend_far(*far, state, [slots[i] for i in FAR])
    parts = lax.all_to_all(parts, ("zl", "y", "c"), 0, 0, tiled=True)
    partial, logs = merge(core, parts, w_out, w_other)
    tiles = lax.all_to_all(partial, "x", 0, 0, tiled=True)
    logs = logs.reshape(2, 2, 2, 2, BLK // 2)
    mine_logs = lax.dynamic_index_in_dim(logs, core, 0, keepdims=False)
    other_logs = lax.ppermute(
        lax.dynamic_index_in_dim(logs, 1 - core, 0, keepdims=False), "c", [(0, 1), (1, 0)]
    )
    ordered = jnp.where(
        core == 0, jnp.stack([mine_logs, other_logs]), jnp.stack([other_logs, mine_logs])
    )
    log_sums = jnp.transpose(ordered, (3, 1, 2, 0, 4)).reshape(2, ROWS)
    output = jnp.sum(tiles.astype(f32), axis=0)
    return (output.astype(bf16), log_sums)


def solution(mesh):
    fine = Mesh(mesh.devices.reshape(8, 2, 4, 4, 2), ("zh", "zl", "y", "x", "c"))
    kv = ("zh", "zl", "y")
    tp = ("x", "c")
    placed = (P(kv, None), P(None, tp), P(None, tp), P(None, tp), P(tp, None), P())
    return jax.shard_map(
        local,
        mesh=fine,
        in_specs=placed,
        out_specs=(P(kv + tp, None), P(tp, kv)),
        check_vma=False,
    )
```

```python
import functools

import jax
import jax.numpy as jnp
from jax import lax
from jax.experimental import pallas as pl
from jax.experimental.pallas import tpu as pltpu
from jax.sharding import Mesh
from jax.sharding import PartitionSpec as P

HEAD_DIM = 64
BLK = 64
SEL = 16
ROWS = 256
PER = 4
WIDTH = 128
RING = 8
TEAM = 8
QB = TEAM * PER
MAXP = QB * SEL
UNROLL_BITS = 5
UNROLL = 1 << UNROLL_BITS
NBLK = 256
NEAR = (0, 1, 2, 6, 7)
FAR = (3, 4, 5)
STATS = 16

rotary_base = 500000.0
masked_score = -1e30
f32 = jnp.float32
bf16 = jnp.bfloat16


def pair_lists(chosen_t, zh, mine, pairs_ref):
    i32 = jnp.int32
    rolled = pltpu.roll(chosen_t, (NBLK - zh * QB) & (NBLK - 1), 1)[:, :WIDTH]
    lists = rolled.astype(f32).T[:QB].astype(i32)
    here = (lists >= 0) & (((lists >> 2) & (TEAM - 1)) == mine)
    slot = (zh - (lists >> 5)) & (RING - 1)
    far = (slot >= FAR[0]) & (slot <= FAR[-1])
    order = jnp.where(far, slot - FAR[0], jnp.where(slot > FAR[-1], slot - len(FAR), slot))
    block = lax.broadcasted_iota(i32, (QB, SEL), 0)
    code = (block * 64 + order * PER + (lists & (PER - 1))).astype(f32)
    earlier = lax.broadcasted_iota(i32, (QB, QB), 1) < lax.broadcasted_iota(i32, (QB, QB), 0)
    before = lax.broadcasted_iota(i32, (SEL, SEL), 0) < lax.broadcasted_iota(i32, (SEL, SEL), 1)
    index = lax.broadcasted_iota(i32, (QB, MAXP), 1).astype(f32)
    row = lax.broadcasted_iota(i32, (1, MAXP), 1).astype(f32)
    for k, wanted in enumerate((here & ~far, here & far)):
        one = jnp.where(wanted, 1.0, 0.0)
        inside = jnp.dot(jnp.where(earlier, 1.0, 0.0), one, preferred_element_type=f32)
        sums = jnp.sum(one, axis=0, keepdims=True)
        base = jnp.dot(sums, jnp.where(before, 1.0, 0.0), preferred_element_type=f32)
        place = jnp.where(wanted, inside + base, -1.0)
        picked = jnp.zeros((QB, MAXP), f32)
        for j in range(SEL):
            picked = picked + jnp.where(place[:, j : j + 1] == index, code[:, j : j + 1], 0.0)
        count = jnp.sum(sums, axis=1, keepdims=True)
        pairs = jnp.where(row < count, jnp.sum(picked, axis=0, keepdims=True), float(QB * 64))
        pairs_ref[pl.ds(k, 1), :] = pairs.astype(i32)
        trips = (count.astype(i32) + (UNROLL - 1)) >> UNROLL_BITS
        pairs_ref[pl.ds(2 + k, 1), :] = jnp.broadcast_to(trips, (1, MAXP))


def project_kernel(
    place_ref, x_hbm, wq_hbm, wk_hbm, wv_hbm, chosen_ref, cos_ref, sin_ref, q_ref, kv_ref, pairs_ref, x_buf, w_buf, sems
):
    copies = [pltpu.make_async_copy(x_hbm, x_buf, sems.at[0])]
    for i, w in enumerate((wk_hbm, wv_hbm, wq_hbm)):
        copies.append(pltpu.make_async_copy(w, w_buf.at[i], sems.at[i + 1]))
    for copy in copies:
        copy.start()
    pair_lists(chosen_ref[...], place_ref[0], place_ref[1], pairs_ref)
    cos = cos_ref[...]
    sin = sin_ref[...]
    lane = lax.broadcasted_iota(jnp.int32, (ROWS, WIDTH), 1)
    first = (lane & (HEAD_DIM - 1)) < HEAD_DIM // 2

    def turned(t):
        partner = jnp.where(first, pltpu.roll(t, WIDTH - HEAD_DIM // 2, 1), pltpu.roll(t, HEAD_DIM // 2, 1))
        return t * cos + partner * sin

    copies[0].wait()
    copies[1].wait()
    x = x_buf[...]
    k = jnp.dot(x, w_buf[0], preferred_element_type=f32)
    kv_ref[pl.ds(0, ROWS), :] = turned(k).astype(bf16)
    copies[2].wait()
    v = jnp.dot(x, w_buf[1], preferred_element_type=f32)
    for p in range(ROWS // WIDTH):
        kv_ref[pl.ds(ROWS + p * WIDTH, WIDTH), :] = v[p * WIDTH : (p + 1) * WIDTH].T.astype(bf16)
    copies[3].wait()
    q = jnp.dot(x, w_buf[2], preferred_element_type=f32)
    q = turned(q) * (HEAD_DIM**-0.5)
    for p in range(ROWS // WIDTH):
        flipped = q[p * WIDTH : (p + 1) * WIDTH].T.astype(bf16)
        for i in range(TEAM):
            q_ref[i, pl.ds(p * WIDTH, WIDTH), :] = flipped


def project(place, x, wq, wk, wv, chosen_t, cos, sin):
    x, wq, wk, wv = (pltpu.with_memory_space_constraint(a, pltpu.HBM) for a in (x, wq, wk, wv))
    hbm = pl.BlockSpec(memory_space=pltpu.HBM)
    smem = pl.BlockSpec(memory_space=pltpu.SMEM)
    vmem = pl.BlockSpec(memory_space=pltpu.VMEM)
    return pl.pallas_call(
        project_kernel,
        out_shape=(
            jax.ShapeDtypeStruct((TEAM, ROWS, WIDTH), bf16),
            jax.ShapeDtypeStruct((2 * ROWS, WIDTH), bf16),
            jax.ShapeDtypeStruct((4, MAXP), jnp.int32),
        ),
        in_specs=[smem] + [hbm] * 4 + [vmem] * 3,
        out_specs=(vmem, vmem, vmem),
        scratch_shapes=[
            pltpu.VMEM(x.shape, bf16),
            pltpu.VMEM((3,) + wq.shape, bf16),
            pltpu.SemaphoreType.DMA((4,)),
        ],
        compiler_params=pltpu.CompilerParams(vmem_limit_bytes=12 << 20),
        name="project",
    )(place, x, wq, wk, wv, chosen_t, cos, sin)


def fill_keys(kv_refs, kbuf, vbuf):
    for s, ref in enumerate(kv_refs):
        for b in range(PER):
            kbuf[s * PER + b] = ref[pl.ds(b * BLK, BLK), :]
        for p in range(ROWS // WIDTH):
            both = ref[pl.ds(ROWS + p * WIDTH, WIDTH), :]
            vbuf[s * PER + 2 * p] = both[:, :BLK]
            vbuf[s * PER + 2 * p + 1] = both[:, BLK:]


def fill_queries(q_ref, qq):
    lane = lax.broadcasted_iota(jnp.int32, (WIDTH, WIDTH), 1)
    row = lax.broadcasted_iota(jnp.int32, (WIDTH, WIDTH), 0)
    half = BLK // 2
    own = (row < HEAD_DIM) == ((lane & half) == 0)
    early = lane < half
    late = lane >= 3 * half
    for i in range(TEAM):
        for p in range(ROWS // WIDTH):
            t = q_ref[i, pl.ds(p * WIDTH, WIDTH), :].astype(f32)
            r64 = pltpu.roll(t, 2 * half, 1)
            first = jnp.where(early, t, jnp.where(late, r64, pltpu.roll(t, half, 1)))
            second = jnp.where(early, r64, jnp.where(late, t, pltpu.roll(t, 3 * half, 1)))
            qq[i * PER + 2 * p] = jnp.where(own, first, 0.0).astype(bf16)
            qq[i * PER + 2 * p + 1] = jnp.where(own, second, 0.0).astype(bf16)
    qq[QB] = jnp.zeros((WIDTH, WIDTH), bf16)


def run_pairs(pairs_ref, kind, qq, kbuf, vbuf, sbuf, mbuf, lbuf, acc, rescale):
    even = (lax.broadcasted_iota(jnp.int32, (BLK, WIDTH), 1) & (HEAD_DIM // 2)) == 0
    trips = pairs_ref[2 + kind, 0]

    def score(it, carry):
        for u in range(UNROLL):
            i = it * UNROLL + u
            code = pairs_ref[kind, i]
            qi = code >> 6
            ki = code & 63
            st = jnp.dot(kbuf[ki], qq[qi], preferred_element_type=f32)
            sbuf[i] = st
            m8 = jnp.max(st.reshape(8, 8, WIDTH), axis=0)
            mbuf[qi] = jnp.maximum(mbuf[qi], m8)
        return carry

    lax.fori_loop(0, trips, score, 0)
    for i in range(QB + 1):
        top = jnp.broadcast_to(jnp.max(mbuf[i], axis=0, keepdims=True), (8, WIDTH))
        mbuf[i] = top
        if rescale is not None:
            factor = jnp.exp(rescale[i] - top)
            lbuf[i] = lbuf[i] * factor
            acc[i] = (acc[i].reshape(8, 8, WIDTH) * factor[None]).reshape(BLK, WIDTH)

    def weigh(it, carry):
        for u in range(UNROLL):
            i = it * UNROLL + u
            code = pairs_ref[kind, i]
            qi = code >> 6
            ki = code & 63
            p = jnp.exp(sbuf[i].reshape(8, 8, WIDTH) - mbuf[qi][None])
            lbuf[qi] = lbuf[qi] + jnp.sum(p, axis=0)
            pb = p.reshape(BLK, WIDTH).astype(bf16)
            ot = jnp.dot(vbuf[ki], pb, preferred_element_type=f32)
            acc[qi] = acc[qi] + jnp.where(even, ot[:HEAD_DIM], ot[HEAD_DIM:])
        return carry

    lax.fori_loop(0, trips, weigh, 0)


def near_kernel(pairs_ref, q_ref, *refs):
    n = len(NEAR)
    qq, mbuf, lbuf, acc = refs[n : n + 4]
    kbuf, vbuf, sbuf = refs[n + 4 :]
    fill_keys(refs[:n], kbuf, vbuf)
    fill_queries(q_ref, qq)
    mbuf[...] = jnp.full(mbuf.shape, masked_score, f32)
    lbuf[...] = jnp.zeros(lbuf.shape, f32)
    acc[...] = jnp.zeros(acc.shape, f32)
    run_pairs(pairs_ref, 0, qq, kbuf, vbuf, sbuf, mbuf, lbuf, acc, None)


def far_kernel(pairs_ref, qq, m_ref, l_ref, acc_ref, *refs):
    n = len(FAR)
    out_ref = refs[n]
    kbuf, vbuf, sbuf, mbuf, lbuf, acc = refs[n + 1 :]
    fill_keys(refs[:n], kbuf, vbuf)
    mbuf[...] = m_ref[...]
    lbuf[...] = l_ref[...]
    acc[...] = acc_ref[...]
    run_pairs(pairs_ref, 1, qq, kbuf, vbuf, sbuf, mbuf, lbuf, acc, m_ref)
    for i in range(TEAM):
        logs = []
        for b in range(PER):
            q = i * PER + b
            total = jnp.sum(lbuf[q], axis=0, keepdims=True)
            some = total > 0.0
            safe = jnp.where(some, total, 1.0)
            logs.append(jnp.where(some, mbuf[q, :1, :] + jnp.log(safe), masked_score))
            out_ref[q, pl.ds(0, BLK), :] = (acc[q] * (1.0 / safe)).astype(bf16)
        value = jnp.concatenate(logs, axis=0)
        hi = value.astype(bf16).astype(f32)
        rest = value - hi
        mid = rest.astype(bf16).astype(f32)
        stats = jnp.concatenate([hi, mid, rest - mid, jnp.zeros((PER, WIDTH), f32)], axis=0)
        for b in range(PER):
            out_ref[i * PER + b, pl.ds(BLK, STATS), :] = stats.astype(bf16)


STATE = (
    jax.ShapeDtypeStruct((QB + 1, WIDTH, WIDTH), bf16),
    jax.ShapeDtypeStruct((QB + 1, 8, WIDTH), f32),
    jax.ShapeDtypeStruct((QB + 1, 8, WIDTH), f32),
    jax.ShapeDtypeStruct((QB + 1, BLK, WIDTH), f32),
)


def key_scratch(n):
    return [
        pltpu.VMEM((n * PER, BLK, WIDTH), bf16),
        pltpu.VMEM((n * PER, WIDTH, BLK), bf16),
        pltpu.VMEM((MAXP, BLK, WIDTH), f32),
    ]


def attend_near(pairs, q, kvs):
    smem = pl.BlockSpec(memory_space=pltpu.SMEM)
    vmem = pl.BlockSpec(memory_space=pltpu.VMEM)
    return pl.pallas_call(
        near_kernel,
        out_shape=STATE,
        in_specs=[smem] + [vmem] * (1 + len(kvs)),
        out_specs=(vmem,) * len(STATE),
        scratch_shapes=key_scratch(len(kvs)),
        compiler_params=pltpu.CompilerParams(vmem_limit_bytes=20 << 20),
        name="near",
    )(pairs, q, *kvs)


def attend_far(pairs, state, kvs):
    smem = pl.BlockSpec(memory_space=pltpu.SMEM)
    vmem = pl.BlockSpec(memory_space=pltpu.VMEM)
    return pl.pallas_call(
        far_kernel,
        out_shape=jax.ShapeDtypeStruct((QB, BLK + STATS, WIDTH), bf16),
        in_specs=[smem] + [vmem] * (len(state) + len(kvs)),
        out_specs=vmem,
        scratch_shapes=key_scratch(len(kvs)) + [pltpu.VMEM(s.shape, s.dtype) for s in STATE[1:]],
        compiler_params=pltpu.CompilerParams(vmem_limit_bytes=20 << 20),
        name="far",
    )(pairs, *state, *kvs)


def merge_kernel(place_ref, part_ref, *refs):
    w_refs = refs[:PER]
    own_ref, send_ref, log_ref, att = refs[PER:]
    x = place_ref[0]
    core = place_ref[1]
    half = BLK // 2
    row = lax.broadcasted_iota(jnp.int32, (PER, WIDTH), 0)
    for c in range(PER):
        values = []
        for i in range(TEAM):
            st = part_ref[i * PER + c, pl.ds(BLK, STATS), :].astype(f32)
            values.append(st[:PER] + st[PER : 2 * PER] + st[2 * PER : 3 * PER])
        top = functools.reduce(jnp.maximum, values)
        weights = [jnp.exp(v - top) for v in values]
        total = functools.reduce(jnp.add, weights)

        @pl.when(x == c)
        def _():
            log_ref[...] = top + jnp.log(total)

        inverse = 1.0 / total
        mixed = jnp.zeros((BLK, WIDTH), f32)
        for i in range(TEAM):
            mine = jnp.sum(jnp.where(row == x, weights[i] * inverse, 0.0), axis=0, keepdims=True)
            mixed = mixed + part_ref[i * PER + c, pl.ds(0, BLK), :].astype(f32) * mine
        turned = mixed.T
        for h in range(2):
            heads = [turned[h * BLK + k * half : h * BLK + (k + 1) * half] for k in range(2)]
            att[c, pl.ds(h * half, half), :] = jnp.concatenate(heads, axis=1).astype(bf16)
    y = jnp.dot(att[x], w_refs[0][...], preferred_element_type=f32)
    for k in range(1, PER):
        y = y + jnp.dot(att[(x - k) & (PER - 1)], w_refs[k][...], preferred_element_type=f32)
    own_ref[...] = jnp.where(core == 0, y[:half], y[half:])
    send_ref[...] = jnp.where(core == 0, y[half:], y[:half]).astype(bf16)


def merge(place, parts, w_all):
    smem = pl.BlockSpec(memory_space=pltpu.SMEM)
    vmem = pl.BlockSpec(memory_space=pltpu.VMEM)
    tile = (BLK // 2, w_all[0].shape[-1])
    return pl.pallas_call(
        merge_kernel,
        out_shape=(
            jax.ShapeDtypeStruct(tile, f32),
            jax.ShapeDtypeStruct(tile, bf16),
            jax.ShapeDtypeStruct((PER, WIDTH), f32),
        ),
        in_specs=[smem, vmem] + [vmem] * PER,
        out_specs=(vmem, vmem, vmem),
        scratch_shapes=[pltpu.VMEM((PER, BLK, WIDTH), bf16)],
        compiler_params=pltpu.CompilerParams(vmem_limit_bytes=12 << 20),
        name="merge",
    )(place, parts, *w_all)


def up_pairs(step):
    return [(i, i + 1) for i in range(step - 1, RING - 1)]


def down_pairs(step):
    far = RING // 2 - 1
    return [((r - step + 1) % RING, (r - step) % RING) for r in range(far)]


def local(tokens, w_query, w_key, w_value, w_out, chosen):
    zh = lax.axis_index("zh")
    mine = lax.axis_index(("zl", "y"))
    device = zh * TEAM + mine
    positions = device * ROWS + jnp.arange(ROWS)
    half = HEAD_DIM // 2
    inverse = rotary_base ** (-jnp.arange(half, dtype=f32) / half)
    angles = positions.astype(f32)[:, None] * jnp.tile(inverse, 2 * WIDTH // HEAD_DIM)[None, :]
    sign = jnp.where((jnp.arange(WIDTH) & (HEAD_DIM - 1)) < half, -1.0, 1.0).astype(f32)
    q8, kv, pairs = project(
        jnp.stack([zh, mine]),
        tokens,
        w_query,
        w_key,
        w_value,
        chosen.T,
        jnp.cos(angles),
        jnp.sin(angles) * sign[None, :],
    )
    slots = [kv] + [None] * (RING - 1)
    up = down = kv
    for s in range(1, RING // 2 + 1):
        up = lax.ppermute(up, "zh", up_pairs(s))
        slots[s] = up
        if s < RING // 2:
            down = lax.ppermute(down, "zh", down_pairs(s))
            slots[RING - s] = down
    q_team = lax.all_to_all(q8, ("zl", "y"), 0, 0, tiled=True)
    w_all = [w_out]
    for k in range(1, PER):
        w_all.append(lax.ppermute(w_out, "x", [(i, (i + k) % PER) for i in range(PER)]))
    state = attend_near(pairs, q_team, [slots[i] for i in NEAR])
    parts = attend_far(pairs, state, [slots[i] for i in FAR])
    parts = lax.all_to_all(parts, ("zl", "y", "x"), 0, 0, tiled=True)
    place = jnp.stack([lax.axis_index("x"), lax.axis_index("c")])
    own, send, logs = merge(place, parts, w_all)
    received = lax.ppermute(send, "c", [(0, 1), (1, 0)])
    output = (own + received.astype(f32)).astype(bf16)
    log_sums = jnp.transpose(logs.reshape(PER, 2, 2, BLK // 2), (2, 0, 1, 3)).reshape(2, ROWS)
    return (output, log_sums)


def solution(mesh):
    fine = Mesh(mesh.devices.reshape(8, 2, 4, 4, 2), ("zh", "zl", "y", "x", "c"))
    kv = ("zh", "zl", "y")
    tp = ("x", "c")
    placed = (P(kv, None), P(None, tp), P(None, tp), P(None, tp), P(tp, None), P())
    return jax.shard_map(
        local,
        mesh=fine,
        in_specs=placed,
        out_specs=(P(kv + tp, None), P(tp, kv)),
        check_vma=False,
    )
```

```python
import functools

import jax
import jax.numpy as jnp
from jax import lax
from jax.experimental import pallas as pl
from jax.experimental.pallas import tpu as pltpu
from jax.sharding import Mesh
from jax.sharding import PartitionSpec as P

HEAD_DIM = 64
BLK = 64
SEL = 16
ROWS = 256
PER = 4
WIDTH = 128
RING = 8
TEAM = 8
QB = TEAM * PER
MAXP = QB * SEL
UNROLL_BITS = 5
UNROLL = 1 << UNROLL_BITS
NBLK = 256
NEAR = (0, 1, 2, 6, 7)
FAR = (3, 4, 5)
STATS = 16

rotary_base = 500000.0
masked_score = -1e30
f32 = jnp.float32
bf16 = jnp.bfloat16


def split_lists(chosen_t, zh, mine):
    i32 = jnp.int32
    rolled = pltpu.roll(chosen_t, (NBLK - zh * QB) & (NBLK - 1), 1)[:, :WIDTH]
    lists = rolled.astype(f32).T[:QB].astype(i32)
    here = (lists >= 0) & (((lists >> 2) & (TEAM - 1)) == mine)
    slot = (zh - (lists >> 5)) & (RING - 1)
    far = (slot >= FAR[0]) & (slot <= FAR[-1])
    order = jnp.where(far, slot - FAR[0], jnp.where(slot > FAR[-1], slot - len(FAR), slot))
    block = lax.broadcasted_iota(i32, (QB, SEL), 0)
    code = (block * 64 + order * PER + (lists & (PER - 1))).astype(f32)
    return (here & ~far, here & far), code


def pair_list(lists, kind, pairs_ref):
    i32 = jnp.int32
    wanted, code = lists[0][kind], lists[1]
    earlier = lax.broadcasted_iota(i32, (QB, QB), 1) < lax.broadcasted_iota(i32, (QB, QB), 0)
    before = lax.broadcasted_iota(i32, (SEL, SEL), 0) < lax.broadcasted_iota(i32, (SEL, SEL), 1)
    index = lax.broadcasted_iota(i32, (QB, MAXP), 1).astype(f32)
    row = lax.broadcasted_iota(i32, (1, MAXP), 1).astype(f32)
    one = jnp.where(wanted, 1.0, 0.0)
    inside = jnp.dot(jnp.where(earlier, 1.0, 0.0), one, preferred_element_type=f32)
    sums = jnp.sum(one, axis=0, keepdims=True)
    base = jnp.dot(sums, jnp.where(before, 1.0, 0.0), preferred_element_type=f32)
    place = jnp.where(wanted, inside + base, -1.0)
    picked = jnp.zeros((QB, MAXP), f32)
    for j in range(SEL):
        picked = picked + jnp.where(place[:, j : j + 1] == index, code[:, j : j + 1], 0.0)
    count = jnp.sum(sums, axis=1, keepdims=True)
    pairs = jnp.where(row < count, jnp.sum(picked, axis=0, keepdims=True), float(QB * 64))
    pairs_ref[pl.ds(kind, 1), :] = pairs.astype(i32)
    trips = (count.astype(i32) + (UNROLL - 1)) >> UNROLL_BITS
    pairs_ref[pl.ds(2 + kind, 1), :] = jnp.broadcast_to(trips, (1, MAXP))


def project_kernel(place_ref, *refs):
    x_hbm, wq_hbm, wk_hbm, wv_hbm, chosen_hbm, cos_ref, sin_ref = refs[:7]
    q_hbm, kv_ref, pairs_ref = refs[7:10]
    x_buf, wq_buf, wkv_buf, chosen_buf, q_buf, sems = refs[10:]
    sources = (
        (chosen_hbm, chosen_buf),
        (x_hbm, x_buf),
        (wq_hbm, wq_buf),
        (wk_hbm, wkv_buf.at[:, pl.ds(0, WIDTH)]),
        (wv_hbm, wkv_buf.at[:, pl.ds(WIDTH, WIDTH)]),
    )
    copies = [pltpu.make_async_copy(a, b, sems.at[i]) for i, (a, b) in enumerate(sources)]
    sends = [pltpu.make_async_copy(q_buf, q_hbm.at[i], sems.at[len(copies) + i]) for i in range(TEAM)]
    for copy in copies:
        copy.start()
    cos = cos_ref[...]
    sin = sin_ref[...]
    lane = lax.broadcasted_iota(jnp.int32, (ROWS, WIDTH), 1)
    first = (lane & (HEAD_DIM - 1)) < HEAD_DIM // 2

    def turned(t):
        partner = jnp.where(first, pltpu.roll(t, WIDTH - HEAD_DIM // 2, 1), pltpu.roll(t, HEAD_DIM // 2, 1))
        return t * cos + partner * sin

    copies[0].wait()
    lists = split_lists(chosen_buf[...], place_ref[0], place_ref[1])
    pair_list(lists, 0, pairs_ref)
    copies[1].wait()
    copies[2].wait()
    q = jnp.dot(x_buf[...], wq_buf[...], preferred_element_type=f32)
    q = turned(q) * (HEAD_DIM**-0.5)
    for p in range(ROWS // WIDTH):
        q_buf[pl.ds(p * WIDTH, WIDTH), :] = q[p * WIDTH : (p + 1) * WIDTH].T.astype(bf16)
    for send in sends:
        send.start()
    copies[3].wait()
    copies[4].wait()
    kv = jnp.dot(x_buf[...], wkv_buf[...], preferred_element_type=f32)
    pair_list(lists, 1, pairs_ref)
    kv_ref[pl.ds(0, ROWS), :] = turned(kv[:, :WIDTH]).astype(bf16)
    for p in range(ROWS // WIDTH):
        kv_ref[pl.ds(ROWS + p * WIDTH, WIDTH), :] = kv[p * WIDTH : (p + 1) * WIDTH, WIDTH:].T.astype(bf16)
    for send in sends:
        send.wait()


def project(place, x, wq, wk, wv, chosen_t, cos, sin):
    x, wq, wk, wv, chosen_t = (
        pltpu.with_memory_space_constraint(a, pltpu.HBM) for a in (x, wq, wk, wv, chosen_t)
    )
    hbm = pl.BlockSpec(memory_space=pltpu.HBM)
    smem = pl.BlockSpec(memory_space=pltpu.SMEM)
    vmem = pl.BlockSpec(memory_space=pltpu.VMEM)
    return pl.pallas_call(
        project_kernel,
        out_shape=(
            jax.ShapeDtypeStruct((TEAM, ROWS, WIDTH), bf16),
            jax.ShapeDtypeStruct((2 * ROWS, WIDTH), bf16),
            jax.ShapeDtypeStruct((4, MAXP), jnp.int32),
        ),
        in_specs=[smem] + [hbm] * 5 + [vmem] * 2,
        out_specs=(pl.BlockSpec(memory_space=pl.ANY), vmem, vmem),
        scratch_shapes=[
            pltpu.VMEM(x.shape, bf16),
            pltpu.VMEM(wq.shape, bf16),
            pltpu.VMEM((wk.shape[0], 2 * WIDTH), bf16),
            pltpu.VMEM(chosen_t.shape, jnp.int32),
            pltpu.VMEM((ROWS, WIDTH), bf16),
            pltpu.SemaphoreType.DMA((5 + TEAM,)),
        ],
        compiler_params=pltpu.CompilerParams(vmem_limit_bytes=12 << 20),
        name="project",
    )(place, x, wq, wk, wv, chosen_t, cos, sin)


def fill_keys(kv_refs, kbuf, vbuf):
    for s, ref in enumerate(kv_refs):
        for b in range(PER):
            kbuf[s * PER + b] = ref[pl.ds(b * BLK, BLK), :]
        for p in range(ROWS // WIDTH):
            both = ref[pl.ds(ROWS + p * WIDTH, WIDTH), :]
            vbuf[s * PER + 2 * p] = both[:, :BLK]
            vbuf[s * PER + 2 * p + 1] = both[:, BLK:]


def fill_queries(q_ref, qq):
    lane = lax.broadcasted_iota(jnp.int32, (WIDTH, WIDTH), 1)
    row = lax.broadcasted_iota(jnp.int32, (WIDTH, WIDTH), 0)
    half = BLK // 2
    own = (row < HEAD_DIM) == ((lane & half) == 0)
    early = lane < half
    late = lane >= 3 * half
    for i in range(TEAM):
        for p in range(ROWS // WIDTH):
            t = q_ref[i, pl.ds(p * WIDTH, WIDTH), :].astype(f32)
            r64 = pltpu.roll(t, 2 * half, 1)
            first = jnp.where(early, t, jnp.where(late, r64, pltpu.roll(t, half, 1)))
            second = jnp.where(early, r64, jnp.where(late, t, pltpu.roll(t, 3 * half, 1)))
            qq[i * PER + 2 * p] = jnp.where(own, first, 0.0).astype(bf16)
            qq[i * PER + 2 * p + 1] = jnp.where(own, second, 0.0).astype(bf16)
    qq[QB] = jnp.zeros((WIDTH, WIDTH), bf16)


def run_pairs(pairs_ref, kind, qq, kbuf, vbuf, sbuf, mbuf, lbuf, acc, rescale):
    even = (lax.broadcasted_iota(jnp.int32, (BLK, WIDTH), 1) & (HEAD_DIM // 2)) == 0
    trips = pairs_ref[2 + kind, 0]

    def score(it, carry):
        for u in range(UNROLL):
            i = it * UNROLL + u
            code = pairs_ref[kind, i]
            qi = code >> 6
            ki = code & 63
            st = jnp.dot(kbuf[ki], qq[qi], preferred_element_type=f32)
            sbuf[i] = st
            m8 = jnp.max(st.reshape(8, 8, WIDTH), axis=0)
            mbuf[qi] = jnp.maximum(mbuf[qi], m8)
        return carry

    lax.fori_loop(0, trips, score, 0)
    for i in range(QB + 1):
        top = jnp.broadcast_to(jnp.max(mbuf[i], axis=0, keepdims=True), (8, WIDTH))
        mbuf[i] = top
        if rescale is not None:
            factor = jnp.exp(rescale[i] - top)
            lbuf[i] = lbuf[i] * factor
            acc[i] = (acc[i].reshape(8, 8, WIDTH) * factor[None]).reshape(BLK, WIDTH)

    def weigh(it, carry):
        for u in range(UNROLL):
            i = it * UNROLL + u
            code = pairs_ref[kind, i]
            qi = code >> 6
            ki = code & 63
            p = jnp.exp(sbuf[i].reshape(8, 8, WIDTH) - mbuf[qi][None])
            lbuf[qi] = lbuf[qi] + jnp.sum(p, axis=0)
            pb = p.reshape(BLK, WIDTH).astype(bf16)
            ot = jnp.dot(vbuf[ki], pb, preferred_element_type=f32)
            acc[qi] = acc[qi] + jnp.where(even, ot[:HEAD_DIM], ot[HEAD_DIM:])
        return carry

    lax.fori_loop(0, trips, weigh, 0)


def near_kernel(pairs_ref, q_ref, *refs):
    n = len(NEAR)
    qq, mbuf, lbuf, acc = refs[n : n + 4]
    kbuf, vbuf, sbuf = refs[n + 4 :]
    fill_keys(refs[:n], kbuf, vbuf)
    fill_queries(q_ref, qq)
    mbuf[...] = jnp.full(mbuf.shape, masked_score, f32)
    lbuf[...] = jnp.zeros(lbuf.shape, f32)
    acc[...] = jnp.zeros(acc.shape, f32)
    run_pairs(pairs_ref, 0, qq, kbuf, vbuf, sbuf, mbuf, lbuf, acc, None)


def far_kernel(pairs_ref, qq, m_ref, l_ref, acc_ref, *refs):
    n = len(FAR)
    out_hbm = refs[n]
    kbuf, vbuf, sbuf, mbuf, lbuf, acc, out_buf, sems = refs[n + 1 :]
    fill_keys(refs[:n], kbuf, vbuf)
    mbuf[...] = m_ref[...]
    lbuf[...] = l_ref[...]
    acc[...] = acc_ref[...]
    run_pairs(pairs_ref, 1, qq, kbuf, vbuf, sbuf, mbuf, lbuf, acc, m_ref)
    sends = []
    for i in range(TEAM):
        logs = []
        for b in range(PER):
            q = i * PER + b
            total = jnp.sum(lbuf[q], axis=0, keepdims=True)
            some = total > 0.0
            safe = jnp.where(some, total, 1.0)
            logs.append(jnp.where(some, mbuf[q, :1, :] + jnp.log(safe), masked_score))
            out_buf[q, pl.ds(0, BLK), :] = (acc[q] * (1.0 / safe)).astype(bf16)
        value = jnp.concatenate(logs, axis=0)
        hi = value.astype(bf16).astype(f32)
        rest = value - hi
        mid = rest.astype(bf16).astype(f32)
        stats = jnp.concatenate([hi, mid, rest - mid, jnp.zeros((PER, WIDTH), f32)], axis=0)
        for b in range(PER):
            out_buf[i * PER + b, pl.ds(BLK, STATS), :] = stats.astype(bf16)
        span = pl.ds(i * PER, PER)
        sends.append(pltpu.make_async_copy(out_buf.at[span], out_hbm.at[span], sems.at[i]))
        sends[-1].start()
    for send in sends:
        send.wait()


STATE = (
    jax.ShapeDtypeStruct((QB + 1, WIDTH, WIDTH), bf16),
    jax.ShapeDtypeStruct((QB + 1, 8, WIDTH), f32),
    jax.ShapeDtypeStruct((QB + 1, 8, WIDTH), f32),
    jax.ShapeDtypeStruct((QB + 1, BLK, WIDTH), f32),
)


def key_scratch(n):
    return [
        pltpu.VMEM((n * PER, BLK, WIDTH), bf16),
        pltpu.VMEM((n * PER, WIDTH, BLK), bf16),
        pltpu.VMEM((MAXP, BLK, WIDTH), f32),
    ]


def attend_near(pairs, q, kvs):
    smem = pl.BlockSpec(memory_space=pltpu.SMEM)
    vmem = pl.BlockSpec(memory_space=pltpu.VMEM)
    return pl.pallas_call(
        near_kernel,
        out_shape=STATE,
        in_specs=[smem] + [vmem] * (1 + len(kvs)),
        out_specs=(vmem,) * len(STATE),
        scratch_shapes=key_scratch(len(kvs)),
        compiler_params=pltpu.CompilerParams(vmem_limit_bytes=20 << 20),
        name="near",
    )(pairs, q, *kvs)


def attend_far(pairs, state, kvs):
    smem = pl.BlockSpec(memory_space=pltpu.SMEM)
    vmem = pl.BlockSpec(memory_space=pltpu.VMEM)
    return pl.pallas_call(
        far_kernel,
        out_shape=jax.ShapeDtypeStruct((QB, BLK + STATS, WIDTH), bf16),
        in_specs=[smem] + [vmem] * (len(state) + len(kvs)),
        out_specs=pl.BlockSpec(memory_space=pl.ANY),
        scratch_shapes=key_scratch(len(kvs))
        + [pltpu.VMEM(s.shape, s.dtype) for s in STATE[1:]]
        + [pltpu.VMEM((QB, BLK + STATS, WIDTH), bf16), pltpu.SemaphoreType.DMA((TEAM,))],
        compiler_params=pltpu.CompilerParams(vmem_limit_bytes=20 << 20),
        name="far",
    )(pairs, *state, *kvs)


def merge_kernel(place_ref, part_ref, *refs):
    w_refs = refs[:PER]
    own_ref, send_ref, log_ref, att = refs[PER:]
    x = place_ref[0]
    core = place_ref[1]
    half = BLK // 2
    row = lax.broadcasted_iota(jnp.int32, (PER, WIDTH), 0)
    for c in range(PER):
        values = []
        for i in range(TEAM):
            st = part_ref[i * PER + c, pl.ds(BLK, STATS), :].astype(f32)
            values.append(st[:PER] + st[PER : 2 * PER] + st[2 * PER : 3 * PER])
        top = functools.reduce(jnp.maximum, values)
        weights = [jnp.exp(v - top) for v in values]
        total = functools.reduce(jnp.add, weights)

        @pl.when(x == c)
        def _():
            log_ref[...] = top + jnp.log(total)

        inverse = 1.0 / total
        mixed = jnp.zeros((BLK, WIDTH), f32)
        for i in range(TEAM):
            mine = jnp.sum(jnp.where(row == x, weights[i] * inverse, 0.0), axis=0, keepdims=True)
            mixed = mixed + part_ref[i * PER + c, pl.ds(0, BLK), :].astype(f32) * mine
        turned = mixed.T
        for h in range(2):
            heads = [turned[h * BLK + k * half : h * BLK + (k + 1) * half] for k in range(2)]
            att[c, pl.ds(h * half, half), :] = jnp.concatenate(heads, axis=1).astype(bf16)
    y = jnp.dot(att[x], w_refs[0][...], preferred_element_type=f32)
    for k in range(1, PER):
        y = y + jnp.dot(att[(x - k) & (PER - 1)], w_refs[k][...], preferred_element_type=f32)
    own_ref[...] = jnp.where(core == 0, y[:half], y[half:])
    send_ref[...] = jnp.where(core == 0, y[half:], y[:half]).astype(bf16)


def merge(place, parts, w_all):
    smem = pl.BlockSpec(memory_space=pltpu.SMEM)
    vmem = pl.BlockSpec(memory_space=pltpu.VMEM)
    tile = (BLK // 2, w_all[0].shape[-1])
    return pl.pallas_call(
        merge_kernel,
        out_shape=(
            jax.ShapeDtypeStruct(tile, f32),
            jax.ShapeDtypeStruct(tile, bf16),
            jax.ShapeDtypeStruct((PER, WIDTH), f32),
        ),
        in_specs=[smem, vmem] + [vmem] * PER,
        out_specs=(vmem, vmem, vmem),
        scratch_shapes=[pltpu.VMEM((PER, BLK, WIDTH), bf16)],
        compiler_params=pltpu.CompilerParams(vmem_limit_bytes=12 << 20),
        name="merge",
    )(place, parts, *w_all)


def up_pairs(step):
    return [(i, i + 1) for i in range(step - 1, RING - 1)]


def down_pairs(step):
    far = RING // 2 - 1
    return [((r - step + 1) % RING, (r - step) % RING) for r in range(far)]


def local(tokens, w_query, w_key, w_value, w_out, chosen):
    zh = lax.axis_index("zh")
    mine = lax.axis_index(("zl", "y"))
    device = zh * TEAM + mine
    positions = device * ROWS + jnp.arange(ROWS)
    half = HEAD_DIM // 2
    inverse = rotary_base ** (-jnp.arange(half, dtype=f32) / half)
    angles = positions.astype(f32)[:, None] * jnp.tile(inverse, 2 * WIDTH // HEAD_DIM)[None, :]
    sign = jnp.where((jnp.arange(WIDTH) & (HEAD_DIM - 1)) < half, -1.0, 1.0).astype(f32)
    q8, kv, pairs = project(
        jnp.stack([zh, mine]),
        tokens,
        w_query,
        w_key,
        w_value,
        chosen.T,
        jnp.cos(angles),
        jnp.sin(angles) * sign[None, :],
    )
    slots = [kv] + [None] * (RING - 1)
    up = down = kv
    for s in range(1, RING // 2 + 1):
        up = lax.ppermute(up, "zh", up_pairs(s))
        slots[s] = up
        if s < RING // 2:
            down = lax.ppermute(down, "zh", down_pairs(s))
            slots[RING - s] = down
    q_team = lax.all_to_all(q8, ("zl", "y"), 0, 0, tiled=True)
    w_all = [w_out]
    for k in range(1, PER):
        w_all.append(lax.ppermute(w_out, "x", [(i, (i + k) % PER) for i in range(PER)]))
    state = attend_near(pairs, q_team, [slots[i] for i in NEAR])
    parts = attend_far(pairs, state, [slots[i] for i in FAR])
    parts = lax.all_to_all(parts, ("zl", "y", "x"), 0, 0, tiled=True)
    place = jnp.stack([lax.axis_index("x"), lax.axis_index("c")])
    own, send, logs = merge(place, parts, w_all)
    received = lax.ppermute(send, "c", [(0, 1), (1, 0)])
    output = (own + received.astype(f32)).astype(bf16)
    log_sums = jnp.transpose(logs.reshape(PER, 2, 2, BLK // 2), (2, 0, 1, 3)).reshape(2, ROWS)
    return (output, log_sums)


def solution(mesh):
    fine = Mesh(mesh.devices.reshape(8, 2, 4, 4, 2), ("zh", "zl", "y", "x", "c"))
    kv = ("zh", "zl", "y")
    tp = ("x", "c")
    placed = (P(kv, None), P(None, tp), P(None, tp), P(None, tp), P(tp, None), P())
    return jax.shard_map(
        local,
        mesh=fine,
        in_specs=placed,
        out_specs=(P(kv + tp, None), P(tp, kv)),
        check_vma=False,
    )
```

```python
import functools

import jax
import jax.numpy as jnp
from jax import lax
from jax.experimental import pallas as pl
from jax.experimental.pallas import tpu as pltpu
from jax.sharding import Mesh
from jax.sharding import PartitionSpec as P

HEAD_DIM = 64
BLK = 64
SEL = 16
ROWS = 256
PER = 4
WIDTH = 128
RING = 8
TEAM = 8
QB = TEAM * PER
MAXP = QB * SEL
UNROLL_BITS = (5, 4)
NBLK = 256
NEAR = (0, 1, 2, 3, 6, 7)
FAR = (4, 5)
STATS = 16

rotary_base = 500000.0
masked_score = -1e30
f32 = jnp.float32
bf16 = jnp.bfloat16


def split_lists(chosen_t, zh, mine):
    i32 = jnp.int32
    rolled = pltpu.roll(chosen_t, (NBLK - zh * QB) & (NBLK - 1), 1)[:, :WIDTH]
    lists = rolled.astype(f32).T[:QB].astype(i32)
    here = (lists >= 0) & (((lists >> 2) & (TEAM - 1)) == mine)
    slot = (zh - (lists >> 5)) & (RING - 1)
    far = (slot >= FAR[0]) & (slot <= FAR[-1])
    order = jnp.where(far, slot - FAR[0], jnp.where(slot > FAR[-1], slot - len(FAR), slot))
    block = lax.broadcasted_iota(i32, (QB, SEL), 0)
    code = (block * 64 + order * PER + (lists & (PER - 1))).astype(f32)
    return (here & ~far, here & far), code


def pair_list(lists, kind, pairs_ref):
    i32 = jnp.int32
    wanted, code = lists[0][kind], lists[1]
    earlier = lax.broadcasted_iota(i32, (QB, QB), 1) < lax.broadcasted_iota(i32, (QB, QB), 0)
    before = lax.broadcasted_iota(i32, (SEL, SEL), 0) < lax.broadcasted_iota(i32, (SEL, SEL), 1)
    index = lax.broadcasted_iota(i32, (QB, MAXP), 1).astype(f32)
    row = lax.broadcasted_iota(i32, (1, MAXP), 1).astype(f32)
    one = jnp.where(wanted, 1.0, 0.0)
    inside = jnp.dot(jnp.where(earlier, 1.0, 0.0), one, preferred_element_type=f32)
    sums = jnp.sum(one, axis=0, keepdims=True)
    base = jnp.dot(sums, jnp.where(before, 1.0, 0.0), preferred_element_type=f32)
    place = jnp.where(wanted, inside + base, -1.0)
    picked = jnp.zeros((QB, MAXP), f32)
    for j in range(SEL):
        picked = picked + jnp.where(place[:, j : j + 1] == index, code[:, j : j + 1], 0.0)
    count = jnp.sum(sums, axis=1, keepdims=True)
    pairs = jnp.where(row < count, jnp.sum(picked, axis=0, keepdims=True), float(QB * 64))
    pairs_ref[pl.ds(kind, 1), :] = pairs.astype(i32)
    trips = (count.astype(i32) + ((1 << UNROLL_BITS[kind]) - 1)) >> UNROLL_BITS[kind]
    pairs_ref[pl.ds(2 + kind, 1), :] = jnp.broadcast_to(trips, (1, MAXP))


def project_kernel(place_ref, *refs):
    x_hbm, wq_hbm, wk_hbm, wv_hbm, chosen_hbm, cos_ref, sin_ref = refs[:7]
    q_hbm, kv_ref, pairs_ref = refs[7:10]
    x_buf, wq_buf, wkv_buf, chosen_buf, q_buf, sems = refs[10:]
    sources = (
        (chosen_hbm, chosen_buf),
        (x_hbm, x_buf),
        (wq_hbm, wq_buf),
        (wk_hbm, wkv_buf.at[:, pl.ds(0, WIDTH)]),
        (wv_hbm, wkv_buf.at[:, pl.ds(WIDTH, WIDTH)]),
    )
    copies = [pltpu.make_async_copy(a, b, sems.at[i]) for i, (a, b) in enumerate(sources)]
    sends = [pltpu.make_async_copy(q_buf, q_hbm.at[i], sems.at[len(copies) + i]) for i in range(TEAM)]
    for copy in copies:
        copy.start()
    cos = cos_ref[...]
    sin = sin_ref[...]
    lane = lax.broadcasted_iota(jnp.int32, (ROWS, WIDTH), 1)
    first = (lane & (HEAD_DIM - 1)) < HEAD_DIM // 2

    def turned(t):
        partner = jnp.where(first, pltpu.roll(t, WIDTH - HEAD_DIM // 2, 1), pltpu.roll(t, HEAD_DIM // 2, 1))
        return t * cos + partner * sin

    copies[0].wait()
    lists = split_lists(chosen_buf[...], place_ref[0], place_ref[1])
    pair_list(lists, 0, pairs_ref)
    copies[1].wait()
    copies[2].wait()
    q = jnp.dot(x_buf[...], wq_buf[...], preferred_element_type=f32)
    q = turned(q) * (HEAD_DIM**-0.5)
    for p in range(ROWS // WIDTH):
        q_buf[pl.ds(p * WIDTH, WIDTH), :] = q[p * WIDTH : (p + 1) * WIDTH].T.astype(bf16)
    for send in sends:
        send.start()
    copies[3].wait()
    copies[4].wait()
    kv = jnp.dot(x_buf[...], wkv_buf[...], preferred_element_type=f32)
    pair_list(lists, 1, pairs_ref)
    kv_ref[pl.ds(0, ROWS), :] = turned(kv[:, :WIDTH]).astype(bf16)
    for p in range(ROWS // WIDTH):
        kv_ref[pl.ds(ROWS + p * WIDTH, WIDTH), :] = kv[p * WIDTH : (p + 1) * WIDTH, WIDTH:].T.astype(bf16)
    for send in sends:
        send.wait()


def project(place, x, wq, wk, wv, chosen_t, cos, sin):
    x, wq, wk, wv, chosen_t = (
        pltpu.with_memory_space_constraint(a, pltpu.HBM) for a in (x, wq, wk, wv, chosen_t)
    )
    hbm = pl.BlockSpec(memory_space=pltpu.HBM)
    smem = pl.BlockSpec(memory_space=pltpu.SMEM)
    vmem = pl.BlockSpec(memory_space=pltpu.VMEM)
    return pl.pallas_call(
        project_kernel,
        out_shape=(
            jax.ShapeDtypeStruct((TEAM, ROWS, WIDTH), bf16),
            jax.ShapeDtypeStruct((2 * ROWS, WIDTH), bf16),
            jax.ShapeDtypeStruct((4, MAXP), jnp.int32),
        ),
        in_specs=[smem] + [hbm] * 5 + [vmem] * 2,
        out_specs=(pl.BlockSpec(memory_space=pl.ANY), vmem, vmem),
        scratch_shapes=[
            pltpu.VMEM(x.shape, bf16),
            pltpu.VMEM(wq.shape, bf16),
            pltpu.VMEM((wk.shape[0], 2 * WIDTH), bf16),
            pltpu.VMEM(chosen_t.shape, jnp.int32),
            pltpu.VMEM((ROWS, WIDTH), bf16),
            pltpu.SemaphoreType.DMA((5 + TEAM,)),
        ],
        compiler_params=pltpu.CompilerParams(vmem_limit_bytes=12 << 20),
        name="project",
    )(place, x, wq, wk, wv, chosen_t, cos, sin)


def fill_keys(kv_refs, kbuf, vbuf):
    for s, ref in enumerate(kv_refs):
        for b in range(PER):
            kbuf[s * PER + b] = ref[pl.ds(b * BLK, BLK), :]
        for p in range(ROWS // WIDTH):
            both = ref[pl.ds(ROWS + p * WIDTH, WIDTH), :]
            vbuf[s * PER + 2 * p] = both[:, :BLK]
            vbuf[s * PER + 2 * p + 1] = both[:, BLK:]


def fill_queries(q_ref, qq):
    lane = lax.broadcasted_iota(jnp.int32, (WIDTH, WIDTH), 1)
    row = lax.broadcasted_iota(jnp.int32, (WIDTH, WIDTH), 0)
    half = BLK // 2
    own = (row < HEAD_DIM) == ((lane & half) == 0)
    early = lane < half
    late = lane >= 3 * half
    for i in range(TEAM):
        for p in range(ROWS // WIDTH):
            t = q_ref[i, pl.ds(p * WIDTH, WIDTH), :].astype(f32)
            r64 = pltpu.roll(t, 2 * half, 1)
            first = jnp.where(early, t, jnp.where(late, r64, pltpu.roll(t, half, 1)))
            second = jnp.where(early, r64, jnp.where(late, t, pltpu.roll(t, 3 * half, 1)))
            qq[i * PER + 2 * p] = jnp.where(own, first, 0.0).astype(bf16)
            qq[i * PER + 2 * p + 1] = jnp.where(own, second, 0.0).astype(bf16)
    qq[QB] = jnp.zeros((WIDTH, WIDTH), bf16)


def run_pairs(pairs_ref, kind, qq, kbuf, vbuf, sbuf, mbuf, lbuf, acc, earlier):
    even = (lax.broadcasted_iota(jnp.int32, (BLK, WIDTH), 1) & (HEAD_DIM // 2)) == 0
    trips = pairs_ref[2 + kind, 0]
    unroll = 1 << UNROLL_BITS[kind]

    def score(it, carry):
        for u in range(unroll):
            i = it * unroll + u
            code = pairs_ref[kind, i]
            qi = code >> 6
            ki = code & 63
            st = jnp.dot(kbuf[ki], qq[qi], preferred_element_type=f32)
            sbuf[i] = st
            m8 = jnp.max(st.reshape(8, 8, WIDTH), axis=0)
            mbuf[qi] = jnp.maximum(mbuf[qi], m8)
        return carry

    lax.fori_loop(0, trips, score, 0)
    for i in range(QB + 1):
        top = jnp.broadcast_to(jnp.max(mbuf[i], axis=0, keepdims=True), (8, WIDTH))
        mbuf[i] = top
        if earlier is not None:
            factor = jnp.exp(earlier[0][i] - top)
            lbuf[i] = earlier[1][i] * factor
            acc[i] = (earlier[2][i].reshape(8, 8, WIDTH) * factor[None]).reshape(BLK, WIDTH)

    def weigh(it, carry):
        for u in range(unroll):
            i = it * unroll + u
            code = pairs_ref[kind, i]
            qi = code >> 6
            ki = code & 63
            p = jnp.exp(sbuf[i].reshape(8, 8, WIDTH) - mbuf[qi][None])
            lbuf[qi] = lbuf[qi] + jnp.sum(p, axis=0)
            pb = p.reshape(BLK, WIDTH).astype(bf16)
            ot = jnp.dot(vbuf[ki], pb, preferred_element_type=f32)
            acc[qi] = acc[qi] + jnp.where(even, ot[:HEAD_DIM], ot[HEAD_DIM:])
        return carry

    lax.fori_loop(0, trips, weigh, 0)


def near_kernel(pairs_ref, q_ref, *refs):
    n = len(NEAR)
    qq, mbuf, lbuf, acc = refs[n : n + 4]
    kbuf, vbuf, sbuf = refs[n + 4 :]
    fill_keys(refs[:n], kbuf, vbuf)
    fill_queries(q_ref, qq)
    mbuf[...] = jnp.full(mbuf.shape, masked_score, f32)
    lbuf[...] = jnp.zeros(lbuf.shape, f32)
    acc[...] = jnp.zeros(acc.shape, f32)
    run_pairs(pairs_ref, 0, qq, kbuf, vbuf, sbuf, mbuf, lbuf, acc, None)


def far_kernel(pairs_ref, qq, m_ref, l_ref, acc_ref, *refs):
    n = len(FAR)
    out_hbm = refs[n]
    kbuf, vbuf, sbuf, mbuf, lbuf, acc, out_buf, sems = refs[n + 1 :]
    fill_keys(refs[:n], kbuf, vbuf)
    mbuf[...] = m_ref[...]
    run_pairs(pairs_ref, 1, qq, kbuf, vbuf, sbuf, mbuf, lbuf, acc, (m_ref, l_ref, acc_ref))
    sends = []
    for i in range(TEAM):
        logs = []
        for b in range(PER):
            q = i * PER + b
            total = jnp.sum(lbuf[q], axis=0, keepdims=True)
            some = total > 0.0
            safe = jnp.where(some, total, 1.0)
            logs.append(jnp.where(some, mbuf[q, :1, :] + jnp.log(safe), masked_score))
            out_buf[q, pl.ds(0, BLK), :] = (acc[q] * (1.0 / safe)).astype(bf16)
        value = jnp.concatenate(logs, axis=0)
        hi = value.astype(bf16).astype(f32)
        rest = value - hi
        mid = rest.astype(bf16).astype(f32)
        stats = jnp.concatenate([hi, mid, rest - mid, jnp.zeros((PER, WIDTH), f32)], axis=0)
        for b in range(PER):
            out_buf[i * PER + b, pl.ds(BLK, STATS), :] = stats.astype(bf16)
        span = pl.ds(i * PER, PER)
        sends.append(pltpu.make_async_copy(out_buf.at[span], out_hbm.at[span], sems.at[i]))
        sends[-1].start()
    for send in sends:
        send.wait()


STATE = (
    jax.ShapeDtypeStruct((QB + 1, WIDTH, WIDTH), bf16),
    jax.ShapeDtypeStruct((QB + 1, 8, WIDTH), f32),
    jax.ShapeDtypeStruct((QB + 1, 8, WIDTH), f32),
    jax.ShapeDtypeStruct((QB + 1, BLK, WIDTH), f32),
)


def key_scratch(n):
    return [
        pltpu.VMEM((n * PER, BLK, WIDTH), bf16),
        pltpu.VMEM((n * PER, WIDTH, BLK), bf16),
        pltpu.VMEM((MAXP, BLK, WIDTH), f32),
    ]


def attend_near(pairs, q, kvs):
    smem = pl.BlockSpec(memory_space=pltpu.SMEM)
    vmem = pl.BlockSpec(memory_space=pltpu.VMEM)
    return pl.pallas_call(
        near_kernel,
        out_shape=STATE,
        in_specs=[smem] + [vmem] * (1 + len(kvs)),
        out_specs=(vmem,) * len(STATE),
        scratch_shapes=key_scratch(len(kvs)),
        compiler_params=pltpu.CompilerParams(vmem_limit_bytes=20 << 20),
        name="near",
    )(pairs, q, *kvs)


def attend_far(pairs, state, kvs):
    smem = pl.BlockSpec(memory_space=pltpu.SMEM)
    vmem = pl.BlockSpec(memory_space=pltpu.VMEM)
    return pl.pallas_call(
        far_kernel,
        out_shape=jax.ShapeDtypeStruct((QB, BLK + STATS, WIDTH), bf16),
        in_specs=[smem] + [vmem] * (len(state) + len(kvs)),
        out_specs=pl.BlockSpec(memory_space=pl.ANY),
        scratch_shapes=key_scratch(len(kvs))
        + [pltpu.VMEM(s.shape, s.dtype) for s in STATE[1:]]
        + [pltpu.VMEM((QB, BLK + STATS, WIDTH), bf16), pltpu.SemaphoreType.DMA((TEAM,))],
        compiler_params=pltpu.CompilerParams(vmem_limit_bytes=20 << 20),
        name="far",
    )(pairs, *state, *kvs)


def merge_kernel(place_ref, part_ref, *refs):
    w_refs = refs[:PER]
    own_ref, send_ref, log_ref, att = refs[PER:]
    x = place_ref[0]
    core = place_ref[1]
    half = BLK // 2
    row = lax.broadcasted_iota(jnp.int32, (PER, WIDTH), 0)
    for c in range(PER):
        values = []
        for i in range(TEAM):
            st = part_ref[i * PER + c, pl.ds(BLK, STATS), :].astype(f32)
            values.append(st[:PER] + st[PER : 2 * PER] + st[2 * PER : 3 * PER])
        top = functools.reduce(jnp.maximum, values)
        weights = [jnp.exp(v - top) for v in values]
        total = functools.reduce(jnp.add, weights)

        @pl.when(x == c)
        def _():
            log_ref[...] = top + jnp.log(total)

        inverse = 1.0 / total
        mixed = jnp.zeros((BLK, WIDTH), f32)
        for i in range(TEAM):
            mine = jnp.sum(jnp.where(row == x, weights[i] * inverse, 0.0), axis=0, keepdims=True)
            mixed = mixed + part_ref[i * PER + c, pl.ds(0, BLK), :].astype(f32) * mine
        turned = mixed.T
        for h in range(2):
            heads = [turned[h * BLK + k * half : h * BLK + (k + 1) * half] for k in range(2)]
            att[c, pl.ds(h * half, half), :] = jnp.concatenate(heads, axis=1).astype(bf16)
    y = jnp.dot(att[x], w_refs[0][...], preferred_element_type=f32)
    for k in range(1, PER):
        y = y + jnp.dot(att[(x - k) & (PER - 1)], w_refs[k][...], preferred_element_type=f32)
    own_ref[...] = jnp.where(core == 0, y[:half], y[half:])
    send_ref[...] = jnp.where(core == 0, y[half:], y[:half]).astype(bf16)


def merge(place, parts, w_all):
    smem = pl.BlockSpec(memory_space=pltpu.SMEM)
    vmem = pl.BlockSpec(memory_space=pltpu.VMEM)
    tile = (BLK // 2, w_all[0].shape[-1])
    return pl.pallas_call(
        merge_kernel,
        out_shape=(
            jax.ShapeDtypeStruct(tile, f32),
            jax.ShapeDtypeStruct(tile, bf16),
            jax.ShapeDtypeStruct((PER, WIDTH), f32),
        ),
        in_specs=[smem, vmem] + [vmem] * PER,
        out_specs=(vmem, vmem, vmem),
        scratch_shapes=[pltpu.VMEM((PER, BLK, WIDTH), bf16)],
        compiler_params=pltpu.CompilerParams(vmem_limit_bytes=12 << 20),
        name="merge",
    )(place, parts, *w_all)


def up_pairs(step):
    return [(i, i + 1) for i in range(step - 1, RING - 1)]


def down_pairs(step):
    far = RING // 2 - 1
    return [((r - step + 1) % RING, (r - step) % RING) for r in range(far)]


def local(tokens, w_query, w_key, w_value, w_out, chosen):
    zh = lax.axis_index("zh")
    mine = lax.axis_index(("zl", "y"))
    device = zh * TEAM + mine
    positions = device * ROWS + jnp.arange(ROWS)
    half = HEAD_DIM // 2
    inverse = rotary_base ** (-jnp.arange(half, dtype=f32) / half)
    angles = positions.astype(f32)[:, None] * jnp.tile(inverse, 2 * WIDTH // HEAD_DIM)[None, :]
    sign = jnp.where((jnp.arange(WIDTH) & (HEAD_DIM - 1)) < half, -1.0, 1.0).astype(f32)
    q8, kv, pairs = project(
        jnp.stack([zh, mine]),
        tokens,
        w_query,
        w_key,
        w_value,
        chosen.T,
        jnp.cos(angles),
        jnp.sin(angles) * sign[None, :],
    )
    slots = [kv] + [None] * (RING - 1)
    up = down = kv
    for s in range(1, RING // 2 + 1):
        up = lax.ppermute(up, "zh", up_pairs(s))
        slots[s] = up
        if s < RING // 2:
            down = lax.ppermute(down, "zh", down_pairs(s))
            slots[RING - s] = down
    q_team = lax.all_to_all(q8, ("zl", "y"), 0, 0, tiled=True)
    w_all = [w_out]
    for k in range(1, PER):
        w_all.append(lax.ppermute(w_out, "x", [(i, (i + k) % PER) for i in range(PER)]))
    state = attend_near(pairs, q_team, [slots[i] for i in NEAR])
    parts = attend_far(pairs, state, [slots[i] for i in FAR])
    parts = lax.all_to_all(parts, ("zl", "y", "x"), 0, 0, tiled=True)
    place = jnp.stack([lax.axis_index("x"), lax.axis_index("c")])
    own, send, logs = merge(place, parts, w_all)
    received = lax.ppermute(send, "c", [(0, 1), (1, 0)])
    output = (own + received.astype(f32)).astype(bf16)
    log_sums = jnp.transpose(logs.reshape(PER, 2, 2, BLK // 2), (2, 0, 1, 3)).reshape(2, ROWS)
    return (output, log_sums)


def solution(mesh):
    fine = Mesh(mesh.devices.reshape(8, 2, 4, 4, 2), ("zh", "zl", "y", "x", "c"))
    kv = ("zh", "zl", "y")
    tp = ("x", "c")
    placed = (P(kv, None), P(None, tp), P(None, tp), P(None, tp), P(tp, None), P())
    return jax.shard_map(
        local,
        mesh=fine,
        in_specs=placed,
        out_specs=(P(kv + tp, None), P(tp, kv)),
        check_vma=False,
    )
```

```python
import functools

import jax
import jax.numpy as jnp
from jax import lax
from jax.experimental import pallas as pl
from jax.experimental.pallas import tpu as pltpu
from jax.sharding import Mesh
from jax.sharding import PartitionSpec as P

HEAD_DIM = 64
BLK = 64
SEL = 16
ROWS = 256
PER = 4
WIDTH = 128
RING = 8
TEAM = 8
QB = TEAM * PER
MAXP = QB * SEL
UNROLL_BITS = (5, 4)
NBLK = 256
NEAR = (0, 1, 2, 3, 6, 7)
FAR = (4, 5)
STATS = 16

rotary_base = 500000.0
masked_score = -1e30
f32 = jnp.float32
bf16 = jnp.bfloat16


def split_lists(chosen_t, zh, mine):
    i32 = jnp.int32
    rolled = pltpu.roll(chosen_t, (NBLK - zh * QB) & (NBLK - 1), 1)[:, :WIDTH]
    lists = rolled.astype(f32).T[:QB].astype(i32)
    here = (lists >= 0) & (((lists >> 2) & (TEAM - 1)) == mine)
    slot = (zh - (lists >> 5)) & (RING - 1)
    far = (slot >= FAR[0]) & (slot <= FAR[-1])
    order = jnp.where(far, slot - FAR[0], jnp.where(slot > FAR[-1], slot - len(FAR), slot))
    block = lax.broadcasted_iota(i32, (QB, SEL), 0)
    code = (block * 64 + order * PER + (lists & (PER - 1))).astype(f32)
    return (here & ~far, here & far), code


def pair_list(lists, kind, pairs_ref):
    i32 = jnp.int32
    wanted, code = lists[0][kind], lists[1]
    earlier = lax.broadcasted_iota(i32, (QB, QB), 1) < lax.broadcasted_iota(i32, (QB, QB), 0)
    before = lax.broadcasted_iota(i32, (SEL, SEL), 0) < lax.broadcasted_iota(i32, (SEL, SEL), 1)
    index = lax.broadcasted_iota(i32, (QB, MAXP), 1).astype(f32)
    row = lax.broadcasted_iota(i32, (1, MAXP), 1).astype(f32)
    one = jnp.where(wanted, 1.0, 0.0)
    inside = jnp.dot(jnp.where(earlier, 1.0, 0.0), one, preferred_element_type=f32)
    sums = jnp.sum(one, axis=0, keepdims=True)
    base = jnp.dot(sums, jnp.where(before, 1.0, 0.0), preferred_element_type=f32)
    place = jnp.where(wanted, inside + base, -1.0)
    picked = jnp.zeros((QB, MAXP), f32)
    for j in range(SEL):
        picked = picked + jnp.where(place[:, j : j + 1] == index, code[:, j : j + 1], 0.0)
    count = jnp.sum(sums, axis=1, keepdims=True)
    pairs = jnp.where(row < count, jnp.sum(picked, axis=0, keepdims=True), float(QB * 64))
    pairs_ref[pl.ds(kind, 1), :] = pairs.astype(i32)
    trips = (count.astype(i32) + ((1 << UNROLL_BITS[kind]) - 1)) >> UNROLL_BITS[kind]
    pairs_ref[pl.ds(2 + kind, 1), :] = jnp.broadcast_to(trips, (1, MAXP))


def project_kernel(place_ref, *refs):
    x_hbm, wq_hbm, wk_hbm, wv_hbm, chosen_hbm, cos_ref, sin_ref = refs[:7]
    q_hbm, kv_ref, pairs_ref = refs[7:10]
    x_buf, wq_buf, wkv_buf, chosen_buf, q_buf, sems = refs[10:]
    sources = (
        (chosen_hbm, chosen_buf),
        (x_hbm, x_buf),
        (wq_hbm, wq_buf),
        (wk_hbm, wkv_buf.at[:, pl.ds(0, WIDTH)]),
        (wv_hbm, wkv_buf.at[:, pl.ds(WIDTH, WIDTH)]),
    )
    copies = [pltpu.make_async_copy(a, b, sems.at[i]) for i, (a, b) in enumerate(sources)]
    sends = [pltpu.make_async_copy(q_buf, q_hbm.at[i], sems.at[len(copies) + i]) for i in range(TEAM)]
    for copy in copies:
        copy.start()
    lane = lax.broadcasted_iota(jnp.int32, (ROWS, WIDTH), 1)
    first = (lane & (HEAD_DIM - 1)) < HEAD_DIM // 2
    cos_j, sin_j = cos_ref[pl.ds(ROWS // 8, 8), :], sin_ref[pl.ds(ROWS // 8, 8), :]
    rows = [(cos_ref[pl.ds(i, 1), :], sin_ref[pl.ds(i, 1), :]) for i in range(ROWS // 8)]
    cos = jnp.concatenate([c * cos_j - s * sin_j for c, s in rows], axis=0)
    sin = jnp.concatenate([s * cos_j + c * sin_j for c, s in rows], axis=0)
    sin = jnp.where(first, -sin, sin)

    def turned(t):
        partner = jnp.where(first, pltpu.roll(t, WIDTH - HEAD_DIM // 2, 1), pltpu.roll(t, HEAD_DIM // 2, 1))
        return t * cos + partner * sin

    copies[0].wait()
    lists = split_lists(chosen_buf[...], place_ref[0], place_ref[1])
    pair_list(lists, 0, pairs_ref)
    copies[1].wait()
    copies[2].wait()
    q = jnp.dot(x_buf[...], wq_buf[...], preferred_element_type=f32)
    q = turned(q) * (HEAD_DIM**-0.5)
    for p in range(ROWS // WIDTH):
        q_buf[pl.ds(p * WIDTH, WIDTH), :] = q[p * WIDTH : (p + 1) * WIDTH].T.astype(bf16)
    for send in sends:
        send.start()
    copies[3].wait()
    copies[4].wait()
    kv = jnp.dot(x_buf[...], wkv_buf[...], preferred_element_type=f32)
    pair_list(lists, 1, pairs_ref)
    kv_ref[pl.ds(0, ROWS), :] = turned(kv[:, :WIDTH]).astype(bf16)
    for p in range(ROWS // WIDTH):
        kv_ref[pl.ds(ROWS + p * WIDTH, WIDTH), :] = kv[p * WIDTH : (p + 1) * WIDTH, WIDTH:].T.astype(bf16)
    for send in sends:
        send.wait()


def project(place, x, wq, wk, wv, chosen_t, cos, sin):
    x, wq, wk, wv, chosen_t = (
        pltpu.with_memory_space_constraint(a, pltpu.HBM) for a in (x, wq, wk, wv, chosen_t)
    )
    hbm = pl.BlockSpec(memory_space=pltpu.HBM)
    smem = pl.BlockSpec(memory_space=pltpu.SMEM)
    vmem = pl.BlockSpec(memory_space=pltpu.VMEM)
    return pl.pallas_call(
        project_kernel,
        out_shape=(
            jax.ShapeDtypeStruct((TEAM, ROWS, WIDTH), bf16),
            jax.ShapeDtypeStruct((2 * ROWS, WIDTH), bf16),
            jax.ShapeDtypeStruct((4, MAXP), jnp.int32),
        ),
        in_specs=[smem] + [hbm] * 5 + [vmem] * 2,
        out_specs=(pl.BlockSpec(memory_space=pl.ANY), vmem, vmem),
        scratch_shapes=[
            pltpu.VMEM(x.shape, bf16),
            pltpu.VMEM(wq.shape, bf16),
            pltpu.VMEM((wk.shape[0], 2 * WIDTH), bf16),
            pltpu.VMEM(chosen_t.shape, jnp.int32),
            pltpu.VMEM((ROWS, WIDTH), bf16),
            pltpu.SemaphoreType.DMA((5 + TEAM,)),
        ],
        compiler_params=pltpu.CompilerParams(vmem_limit_bytes=12 << 20),
        name="project",
    )(place, x, wq, wk, wv, chosen_t, cos, sin)


def fill_keys(kv_refs, kbuf, vbuf):
    for s, ref in enumerate(kv_refs):
        for b in range(PER):
            kbuf[s * PER + b] = ref[pl.ds(b * BLK, BLK), :]
        for p in range(ROWS // WIDTH):
            both = ref[pl.ds(ROWS + p * WIDTH, WIDTH), :]
            vbuf[s * PER + 2 * p] = both[:, :BLK]
            vbuf[s * PER + 2 * p + 1] = both[:, BLK:]


def fill_queries(q_ref, qq):
    lane = lax.broadcasted_iota(jnp.int32, (WIDTH, WIDTH), 1)
    row = lax.broadcasted_iota(jnp.int32, (WIDTH, WIDTH), 0)
    half = BLK // 2
    own = (row < HEAD_DIM) == ((lane & half) == 0)
    early = lane < half
    late = lane >= 3 * half
    for i in range(TEAM):
        for p in range(ROWS // WIDTH):
            t = q_ref[i, pl.ds(p * WIDTH, WIDTH), :].astype(f32)
            r64 = pltpu.roll(t, 2 * half, 1)
            first = jnp.where(early, t, jnp.where(late, r64, pltpu.roll(t, half, 1)))
            second = jnp.where(early, r64, jnp.where(late, t, pltpu.roll(t, 3 * half, 1)))
            qq[i * PER + 2 * p] = jnp.where(own, first, 0.0).astype(bf16)
            qq[i * PER + 2 * p + 1] = jnp.where(own, second, 0.0).astype(bf16)
    qq[QB] = jnp.zeros((WIDTH, WIDTH), bf16)


def run_pairs(pairs_ref, kind, qq, kbuf, vbuf, sbuf, mbuf, lbuf, acc, earlier):
    even = (lax.broadcasted_iota(jnp.int32, (BLK, WIDTH), 1) & (HEAD_DIM // 2)) == 0
    trips = pairs_ref[2 + kind, 0]
    unroll = 1 << UNROLL_BITS[kind]

    def score(it, carry):
        for u in range(unroll):
            i = it * unroll + u
            code = pairs_ref[kind, i]
            qi = code >> 6
            ki = code & 63
            st = jnp.dot(kbuf[ki], qq[qi], preferred_element_type=f32)
            sbuf[i] = st
            m8 = jnp.max(st.reshape(8, 8, WIDTH), axis=0)
            mbuf[qi] = jnp.maximum(mbuf[qi], m8)
        return carry

    lax.fori_loop(0, trips, score, 0)
    for i in range(QB + 1):
        top = jnp.broadcast_to(jnp.max(mbuf[i], axis=0, keepdims=True), (8, WIDTH))
        mbuf[i] = top
        if earlier is not None:
            factor = jnp.exp(earlier[0][i] - top)
            lbuf[i] = earlier[1][i] * factor
            acc[i] = (earlier[2][i].reshape(8, 8, WIDTH) * factor[None]).reshape(BLK, WIDTH)

    def weigh(it, carry):
        for u in range(unroll):
            i = it * unroll + u
            code = pairs_ref[kind, i]
            qi = code >> 6
            ki = code & 63
            p = jnp.exp(sbuf[i].reshape(8, 8, WIDTH) - mbuf[qi][None])
            lbuf[qi] = lbuf[qi] + jnp.sum(p, axis=0)
            pb = p.reshape(BLK, WIDTH).astype(bf16)
            ot = jnp.dot(vbuf[ki], pb, preferred_element_type=f32)
            acc[qi] = acc[qi] + jnp.where(even, ot[:HEAD_DIM], ot[HEAD_DIM:])
        return carry

    lax.fori_loop(0, trips, weigh, 0)


def near_kernel(pairs_ref, q_ref, *refs):
    n = len(NEAR)
    qq, mbuf, lbuf, acc = refs[n : n + 4]
    kbuf, vbuf, sbuf = refs[n + 4 :]
    fill_keys(refs[:n], kbuf, vbuf)
    fill_queries(q_ref, qq)
    mbuf[...] = jnp.full(mbuf.shape, masked_score, f32)
    lbuf[...] = jnp.zeros(lbuf.shape, f32)
    acc[...] = jnp.zeros(acc.shape, f32)
    run_pairs(pairs_ref, 0, qq, kbuf, vbuf, sbuf, mbuf, lbuf, acc, None)


def far_kernel(pairs_ref, qq, m_ref, l_ref, acc_ref, *refs):
    n = len(FAR)
    out_hbm = refs[n]
    kbuf, vbuf, sbuf, mbuf, lbuf, acc, out_buf, sems = refs[n + 1 :]
    fill_keys(refs[:n], kbuf, vbuf)
    mbuf[...] = m_ref[...]
    run_pairs(pairs_ref, 1, qq, kbuf, vbuf, sbuf, mbuf, lbuf, acc, (m_ref, l_ref, acc_ref))
    sends = []
    for i in range(TEAM):
        logs = []
        for b in range(PER):
            q = i * PER + b
            total = jnp.sum(lbuf[q], axis=0, keepdims=True)
            some = total > 0.0
            safe = jnp.where(some, total, 1.0)
            logs.append(jnp.where(some, mbuf[q, :1, :] + jnp.log(safe), masked_score))
            out_buf[q, pl.ds(0, BLK), :] = (acc[q] * (1.0 / safe)).astype(bf16)
        value = jnp.concatenate(logs, axis=0)
        hi = value.astype(bf16).astype(f32)
        rest = value - hi
        mid = rest.astype(bf16).astype(f32)
        stats = jnp.concatenate([hi, mid, rest - mid, jnp.zeros((PER, WIDTH), f32)], axis=0)
        for b in range(PER):
            out_buf[i * PER + b, pl.ds(BLK, STATS), :] = stats.astype(bf16)
        span = pl.ds(i * PER, PER)
        sends.append(pltpu.make_async_copy(out_buf.at[span], out_hbm.at[span], sems.at[i]))
        sends[-1].start()
    for send in sends:
        send.wait()


STATE = (
    jax.ShapeDtypeStruct((QB + 1, WIDTH, WIDTH), bf16),
    jax.ShapeDtypeStruct((QB + 1, 8, WIDTH), f32),
    jax.ShapeDtypeStruct((QB + 1, 8, WIDTH), f32),
    jax.ShapeDtypeStruct((QB + 1, BLK, WIDTH), f32),
)


def key_scratch(n):
    return [
        pltpu.VMEM((n * PER, BLK, WIDTH), bf16),
        pltpu.VMEM((n * PER, WIDTH, BLK), bf16),
        pltpu.VMEM((MAXP, BLK, WIDTH), f32),
    ]


def attend_near(pairs, q, kvs):
    smem = pl.BlockSpec(memory_space=pltpu.SMEM)
    vmem = pl.BlockSpec(memory_space=pltpu.VMEM)
    return pl.pallas_call(
        near_kernel,
        out_shape=STATE,
        in_specs=[smem] + [vmem] * (1 + len(kvs)),
        out_specs=(vmem,) * len(STATE),
        scratch_shapes=key_scratch(len(kvs)),
        compiler_params=pltpu.CompilerParams(vmem_limit_bytes=20 << 20),
        name="near",
    )(pairs, q, *kvs)


def attend_far(pairs, state, kvs):
    smem = pl.BlockSpec(memory_space=pltpu.SMEM)
    vmem = pl.BlockSpec(memory_space=pltpu.VMEM)
    return pl.pallas_call(
        far_kernel,
        out_shape=jax.ShapeDtypeStruct((QB, BLK + STATS, WIDTH), bf16),
        in_specs=[smem] + [vmem] * (len(state) + len(kvs)),
        out_specs=pl.BlockSpec(memory_space=pl.ANY),
        scratch_shapes=key_scratch(len(kvs))
        + [pltpu.VMEM(s.shape, s.dtype) for s in STATE[1:]]
        + [pltpu.VMEM((QB, BLK + STATS, WIDTH), bf16), pltpu.SemaphoreType.DMA((TEAM,))],
        compiler_params=pltpu.CompilerParams(vmem_limit_bytes=20 << 20),
        name="far",
    )(pairs, *state, *kvs)


def merge_kernel(place_ref, part_ref, *refs):
    w_refs = refs[:PER]
    own_ref, send_ref, log_ref, att = refs[PER:]
    x = place_ref[0]
    core = place_ref[1]
    half = BLK // 2
    row = lax.broadcasted_iota(jnp.int32, (PER, WIDTH), 0)
    for c in range(PER):
        values = []
        for i in range(TEAM):
            st = part_ref[i * PER + c, pl.ds(BLK, STATS), :].astype(f32)
            values.append(st[:PER] + st[PER : 2 * PER] + st[2 * PER : 3 * PER])
        top = functools.reduce(jnp.maximum, values)
        weights = [jnp.exp(v - top) for v in values]
        total = functools.reduce(jnp.add, weights)

        @pl.when(x == c)
        def _():
            log_ref[...] = top + jnp.log(total)

        inverse = 1.0 / total
        mixed = jnp.zeros((BLK, WIDTH), f32)
        for i in range(TEAM):
            mine = jnp.sum(jnp.where(row == x, weights[i] * inverse, 0.0), axis=0, keepdims=True)
            mixed = mixed + part_ref[i * PER + c, pl.ds(0, BLK), :].astype(f32) * mine
        turned = mixed.T
        for h in range(2):
            heads = [turned[h * BLK + k * half : h * BLK + (k + 1) * half] for k in range(2)]
            att[c, pl.ds(h * half, half), :] = jnp.concatenate(heads, axis=1).astype(bf16)
    y = jnp.dot(att[x], w_refs[0][...], preferred_element_type=f32)
    for k in range(1, PER):
        y = y + jnp.dot(att[(x - k) & (PER - 1)], w_refs[k][...], preferred_element_type=f32)
    own_ref[...] = jnp.where(core == 0, y[:half], y[half:])
    send_ref[...] = jnp.where(core == 0, y[half:], y[:half]).astype(bf16)


def merge(place, parts, w_all):
    smem = pl.BlockSpec(memory_space=pltpu.SMEM)
    vmem = pl.BlockSpec(memory_space=pltpu.VMEM)
    tile = (BLK // 2, w_all[0].shape[-1])
    return pl.pallas_call(
        merge_kernel,
        out_shape=(
            jax.ShapeDtypeStruct(tile, f32),
            jax.ShapeDtypeStruct(tile, bf16),
            jax.ShapeDtypeStruct((PER, WIDTH), f32),
        ),
        in_specs=[smem, vmem] + [vmem] * PER,
        out_specs=(vmem, vmem, vmem),
        scratch_shapes=[pltpu.VMEM((PER, BLK, WIDTH), bf16)],
        compiler_params=pltpu.CompilerParams(vmem_limit_bytes=12 << 20),
        name="merge",
    )(place, parts, *w_all)


def up_pairs(step):
    return [(i, i + 1) for i in range(step - 1, RING - 1)]


def down_pairs(step):
    far = RING // 2 - 1
    return [((r - step + 1) % RING, (r - step) % RING) for r in range(far)]


def local(tokens, w_query, w_key, w_value, w_out, chosen):
    zh = lax.axis_index("zh")
    mine = lax.axis_index(("zl", "y"))
    device = zh * TEAM + mine
    step = jnp.arange(ROWS // 8 + 8)
    positions = jnp.where(step < ROWS // 8, device * ROWS + 8 * step, step - ROWS // 8)
    half = HEAD_DIM // 2
    inverse = rotary_base ** (-jnp.arange(half, dtype=f32) / half)
    angles = positions.astype(f32)[:, None] * jnp.tile(inverse, 2 * WIDTH // HEAD_DIM)[None, :]
    q8, kv, pairs = project(
        jnp.stack([zh, mine]),
        tokens,
        w_query,
        w_key,
        w_value,
        chosen.T,
        jnp.cos(angles),
        jnp.sin(angles),
    )
    slots = [kv] + [None] * (RING - 1)
    up = down = kv
    for s in range(1, RING // 2 + 1):
        up = lax.ppermute(up, "zh", up_pairs(s))
        slots[s] = up
        if s < RING // 2:
            down = lax.ppermute(down, "zh", down_pairs(s))
            slots[RING - s] = down
    q_team = lax.all_to_all(q8, ("zl", "y"), 0, 0, tiled=True)
    w_all = [w_out]
    for k in range(1, PER):
        w_all.append(lax.ppermute(w_out, "x", [(i, (i + k) % PER) for i in range(PER)]))
    state = attend_near(pairs, q_team, [slots[i] for i in NEAR])
    parts = attend_far(pairs, state, [slots[i] for i in FAR])
    parts = lax.all_to_all(parts, ("zl", "y", "x"), 0, 0, tiled=True)
    place = jnp.stack([lax.axis_index("x"), lax.axis_index("c")])
    own, send, logs = merge(place, parts, w_all)
    received = lax.ppermute(send, "c", [(0, 1), (1, 0)])
    output = (own + received.astype(f32)).astype(bf16)
    log_sums = jnp.transpose(logs.reshape(PER, 2, 2, BLK // 2), (2, 0, 1, 3)).reshape(2, ROWS)
    return (output, log_sums)


def solution(mesh):
    fine = Mesh(mesh.devices.reshape(8, 2, 4, 4, 2), ("zh", "zl", "y", "x", "c"))
    kv = ("zh", "zl", "y")
    tp = ("x", "c")
    placed = (P(kv, None), P(None, tp), P(None, tp), P(None, tp), P(tp, None), P())
    return jax.shard_map(
        local,
        mesh=fine,
        in_specs=placed,
        out_specs=(P(kv + tp, None), P(tp, kv)),
        check_vma=False,
    )
```
